32 devices in a mesh: grp: 2 (over y), dp: 2 (over x), kv: 4 (over z), tp: 2 (over core).
Axes of the slice: x: 2, y: 2, z: 4, core: 2. Of those that a mesh axis runs over, the one named last changes fastest.
Arguments:
- tokens: bfloat16 [16, 4096], P('grp', ('dp', 'kv')), parts along dimension 0, may hold values from -40 to 40
- lengths: int32 [16], P(('grp', 'dp')), parts along dimension 0, may hold values from 2 to 512, as said below
- cache_keys: bfloat16 [16, 512, 6, 256], P(('grp', 'dp'), 'kv', 'tp'), parts along dimension 0, may hold values from -6 to 6
- cache_values: bfloat16 [16, 512, 6, 512], P(('grp', 'dp'), 'kv', 'tp'), parts along dimension 0, may hold values from -6 to 6
- cache_igate: float32 [16, 6, 512], P(('grp', 'dp'), 'tp', 'kv'), parts along dimension 0, may hold values from -5 to 250
- cache_fcum: float32 [16, 6, 512], P(('grp', 'dp'), 'tp', 'kv'), parts along dimension 0, may hold values from -130 to 0, as said below
- gain_mix: bfloat16 [4096], replicated, may hold values from 0.099609375 to 1.8984375
- w_query: bfloat16 [4096, 1536], P(('dp', 'kv'), 'tp'), may hold values from -0.09375 to 0.09375
- w_key: bfloat16 [4096, 1536], P(('dp', 'kv'), 'tp'), may hold values from -0.09375 to 0.09375
- w_value: bfloat16 [4096, 3072], P(('dp', 'kv'), 'tp'), may hold values from -0.09375 to 0.09375
- w_gates: bfloat16 [4096, 12], replicated, may hold values from -0.09375 to 0.09375
- w_out: bfloat16 [3072, 4096], P(None, ('dp', 'kv', 'tp')), may hold values from -0.109375 to 0.109375
- gain_ffn: bfloat16 [4096], replicated, may hold values from 0.099609375 to 1.8984375
- w_gate: bfloat16 [4096, 10240], P(None, ('dp', 'kv', 'tp')), may hold values from -0.09375 to 0.09375
- w_up: bfloat16 [4096, 10240], P(None, ('dp', 'kv', 'tp')), may hold values from -0.09375 to 0.09375
- w_down: bfloat16 [10240, 4096], P(('dp', 'kv', 'tp')), may hold values from -0.078125 to 0.078125
Outputs:
- result: bfloat16 [16, 4096], P('grp', ('dp', 'kv', 'tp')), parts along dimension 0
The draws below stay inside these ranges and needn't reach their ends.
There are 2 independent parts, one for each index of `grp`. The reference program is written for one: setup_inputs(seed, part) draws one part's arguments, and reference() takes and returns one part's arrays. A program takes and returns all parts, laid end to end along the dimension named above; an argument that names none is the same for every part. Nothing has to cross between parts.
Inputs may be any that keep to these rules, and one draw needn't show every extreme that they name: Live cache positions of each sequence; the new token takes position lengths; in every draw one sequence has exactly 512. `cache_fcum`: position p holds the sum of the log forget gates of positions 0 to p of its sequence and head; never rising along positions.
All inputs are finite; a program needn't handle non-finite values.
Results may differ from the reference program's by a relative error of at most 0.012.
Values may be sent and summed in bfloat16 or wider, within the bound.
A program may use at most 64 MiB of HBM per device.

```python
import math
import jax
import jax.numpy as jnp
from jax import lax

D = 4096
HEAD_COUNT = 6
QK = 256
V = 512
FF = 10240
POS_DEV = 128
BATCH_SEQUENCES = 8
CACHE_CAPACITY = 512


def draw_tokens(key, part):
    key_noise, key_jitter, key_rows = jax.random.split(key, 3)
    fraction = jnp.arange(D, dtype=jnp.float32) / D
    noise = jnp.clip(jax.random.normal(key_noise, (BATCH_SEQUENCES, D), jnp.float32), -4.0, 4.0)
    column = 0.25 * jnp.exp(math.log(10.0) * fraction)
    jitter = jax.random.uniform(key_jitter, (1, D), jnp.float32, 0.7, 1.3)
    row_scale = jnp.exp(jax.random.uniform(key_rows, (BATCH_SEQUENCES, 1), jnp.float32, math.log(0.5), math.log(2.0)))
    return (noise * column[None, :] * jitter * row_scale).astype(jnp.bfloat16)


def draw_lengths(key, part):
    key_first, key_second, key_pick = jax.random.split(key, 3)
    draw_first = jax.random.randint(key_first, (BATCH_SEQUENCES,), 2, CACHE_CAPACITY + 1)
    draw_second = jax.random.randint(key_second, (BATCH_SEQUENCES,), 2, CACHE_CAPACITY + 1)
    lengths_all = jnp.minimum(draw_first, draw_second)
    chosen = jax.random.randint(key_pick, (), 0, BATCH_SEQUENCES)
    return jnp.where(jnp.arange(BATCH_SEQUENCES) == chosen, CACHE_CAPACITY, lengths_all).astype(jnp.int32)


def draw_cache_igate(key, part):
    key_noise = jax.random.fold_in(key, 0)
    return jax.random.uniform(key_noise, (BATCH_SEQUENCES, HEAD_COUNT, CACHE_CAPACITY), jnp.float32, -5.0, 1.0)


def draw_cache_fcum(key, part):
    key_fast, key_slow, key_quick, key_block, key_jitter, key_location, key_dimension = jax.random.split(key, 7)
    share_fast = 0.5
    is_fast = jax.random.bernoulli(key_fast, share_fast, (BATCH_SEQUENCES, HEAD_COUNT, 1))
    slow_rate = 0.08 * math.log(10.0) / CACHE_CAPACITY * jax.random.uniform(key_slow, (BATCH_SEQUENCES, HEAD_COUNT, 1), jnp.float32, 0.5, 1.5)
    fast_rate = jax.random.uniform(key_quick, (BATCH_SEQUENCES, HEAD_COUNT, 1), jnp.float32, 1.0 / 60.0, 1.0 / 25.0)
    base_rate = jnp.where(is_fast, fast_rate, slow_rate)
    block_factor = jnp.exp(jax.random.uniform(key_block, (BATCH_SEQUENCES, HEAD_COUNT, CACHE_CAPACITY // POS_DEV), jnp.float32, math.log(0.5), math.log(2.0)))
    block_factor = jnp.repeat(block_factor, POS_DEV, axis=2)
    jitter = jax.random.uniform(key_jitter, (BATCH_SEQUENCES, HEAD_COUNT, CACHE_CAPACITY), jnp.float32, 0.5, 1.5)
    forget_falloff = -base_rate * block_factor * jitter
    spike_start = jax.random.randint(key_location, (BATCH_SEQUENCES, HEAD_COUNT, 2), 0, CACHE_CAPACITY)
    spike_length = jnp.log(jax.random.uniform(key_dimension, (BATCH_SEQUENCES, HEAD_COUNT, 2), jnp.float32, 0.5, 0.8))
    match_count = jnp.arange(CACHE_CAPACITY)[None, None, None, :] == spike_start[..., None]
    forget_falloff = forget_falloff + jnp.sum(jnp.where(match_count, spike_length[..., None], 0.0), axis=2)
    return jnp.cumsum(forget_falloff, axis=2)


def raised(result, stream_key, source, target, shards_of, factor):
    owner, partner = [(jnp.arange(result.shape[position]) // (result.shape[position] // shards_of)).reshape([-1 if axis == position else 1 for axis in range(result.ndim)]) for position in (source, target)]
    chosen = jax.random.permutation(stream_key, shards_of)[partner]
    strong = (owner == chosen) | (owner == (partner + shards_of // 2) % shards_of)
    return jnp.where(strong, factor * result, result)


def shard_levels(rng, extent, cuts, least, largest):
    def one(axis_at, shards_of):
        steps = jax.random.uniform(jax.random.fold_in(jax.random.fold_in(rng, 6), axis_at), (shards_of,), jnp.float32, least / len(cuts), largest / len(cuts))
        return jnp.repeat(jnp.exp(steps), extent[axis_at] // shards_of).reshape((-1,) + (1,) * (len(extent) - axis_at - 1))

    gain = one(*cuts[0])
    for cut in cuts[1:]:
        gain = gain * one(*cut)
    return gain


def scatter_about(stream_key, extent, spread, reach, pieces=(), kind=jnp.bfloat16):
    array = spread * jax.random.normal(stream_key, extent, jnp.float32)
    if pieces:
        array = array * shard_levels(stream_key, extent, pieces, -0.22, 0.18)
    return jnp.clip(array, -reach, reach).astype(kind)


def noise_with(key, shape, deviation, reach, cuts, heavy, held_as=jnp.bfloat16):
    drawn = deviation * jax.random.normal(key, shape, jnp.float32)
    if cuts:
        drawn = drawn * shard_levels(key, shape, cuts, -0.22, 0.18)
    return jnp.clip(raised(drawn, jax.random.fold_in(key, 3), *heavy), -reach, reach).astype(held_as)


def setup_inputs(seed: int = 0, part: int = 0) -> dict:
    key_of = jax.random.split(jax.random.key(seed), 17)
    part_keys = jax.random.split(jax.random.fold_in(key_of[16], part), 17)
    return {
        "tokens": draw_tokens(jax.random.fold_in(jax.random.fold_in(key_of[16], part), 71), part),
        "lengths": draw_lengths(jax.random.fold_in(jax.random.fold_in(key_of[16], part), 71), part),
        "cache_keys": scatter_about(part_keys[2], (BATCH_SEQUENCES, CACHE_CAPACITY, HEAD_COUNT, QK), 1.0, 6.0, ((0, 2), (1, 4), (2, 2))),
        "cache_values": scatter_about(part_keys[3], (BATCH_SEQUENCES, CACHE_CAPACITY, HEAD_COUNT, V), 1.0, 6.0, ((0, 2), (1, 4), (2, 2))),
        "cache_igate": draw_cache_igate(jax.random.fold_in(jax.random.fold_in(key_of[16], part), 71), part),
        "cache_fcum": draw_cache_fcum(jax.random.fold_in(jax.random.fold_in(key_of[16], part), 71), part),
        "gain_mix": jnp.clip(1.0 + 0.18 * jax.random.normal(key_of[6], (D,), jnp.float32), 0.099609375, 1.8984375).astype(jnp.bfloat16),
        "w_query": scatter_about(key_of[7], (D, HEAD_COUNT * QK), D ** -0.5, 0.09375, ((0, 8), (1, 2))),
        "w_key": scatter_about(key_of[8], (D, HEAD_COUNT * QK), D ** -0.5, 0.09375, ((0, 8), (1, 2))),
        "w_value": scatter_about(key_of[9], (D, HEAD_COUNT * V), D ** -0.5, 0.09375, ((0, 8), (1, 2))),
        "w_gates": scatter_about(key_of[10], (D, 2 * HEAD_COUNT), D ** -0.5, 0.09375),
        "w_out": scatter_about(key_of[11], (HEAD_COUNT * V, D), (HEAD_COUNT * V) ** -0.5, 0.109375, ((1, 16),)),
        "gain_ffn": jnp.clip(1.0 + 0.18 * jax.random.normal(key_of[12], (D,), jnp.float32), 0.099609375, 1.8984375).astype(jnp.bfloat16),
        "w_gate": scatter_about(key_of[13], (D, FF), D ** -0.5, 0.09375, ((1, 16),)),
        "w_up": scatter_about(key_of[14], (D, FF), D ** -0.5, 0.09375, ((1, 16),)),
        "w_down": noise_with(key_of[15], (FF, D), FF ** -0.5, 0.078125, ((0, 16),), (0, 1, 16, 2.0)),
    }


epsilon = 1e-06
very_low = -1e+30

def reference(tokens, lengths, cache_keys, cache_values, cache_igate, cache_fcum, gain_mix, w_query, w_key, w_value, w_gates, w_out, gain_ffn, w_gate, w_up, w_down):
    token_f32 = tokens.astype(jnp.float32)
    inv_norm = lax.rsqrt(lax.optimization_barrier(jnp.mean(token_f32 * token_f32, axis=1, keepdims=True)) + epsilon)
    scaled = (token_f32 * gain_mix.astype(jnp.float32)[None, :]).astype(jnp.bfloat16)
    query_new = (jnp.dot(scaled, w_query, preferred_element_type=jnp.float32) * inv_norm).astype(jnp.bfloat16).reshape(BATCH_SEQUENCES, HEAD_COUNT, QK)
    new_key = (jnp.dot(scaled, w_key, preferred_element_type=jnp.float32) * inv_norm).astype(jnp.bfloat16).reshape(BATCH_SEQUENCES, HEAD_COUNT, QK)
    new_value = (jnp.dot(scaled, w_value, preferred_element_type=jnp.float32) * inv_norm).astype(jnp.bfloat16).reshape(BATCH_SEQUENCES, HEAD_COUNT, V)
    gates_now = jnp.dot(scaled, w_gates, preferred_element_type=jnp.float32) * inv_norm
    in_gate = gates_now[:, :HEAD_COUNT]
    log_forget = jax.nn.log_sigmoid(gates_now[:, HEAD_COUNT:])
    inv_root = QK ** (-0.5)
    query_f32 = query_new.astype(jnp.float32)

    def one_block(block_index):
        offset = block_index * POS_DEV
        key_block = lax.dynamic_slice_in_dim(cache_keys, offset, POS_DEV, 1).astype(jnp.float32)
        value_block = lax.dynamic_slice_in_dim(cache_values, offset, POS_DEV, 1).astype(jnp.float32)
        gate_block = lax.dynamic_slice_in_dim(cache_igate, offset, POS_DEV, 2)
        fcum_block = lax.dynamic_slice_in_dim(cache_fcum, offset, POS_DEV, 2)
        scores = jnp.einsum('bhk,bphk->bhp', query_f32, key_block) * inv_root
        positions = offset + jnp.arange(POS_DEV, dtype=jnp.int32)
        is_live = positions[None, None, :] < lengths[:, None, None]
        exponent = jnp.where(is_live, gate_block - fcum_block, very_low)
        block_max = lax.optimization_barrier(jnp.max(exponent, axis=2))
        weight = jnp.where(is_live, jnp.exp(exponent - block_max[..., None]), 0.0)
        product = weight * scores
        block_den = lax.optimization_barrier(jnp.sum(product, axis=2))
        block_prob = lax.optimization_barrier(product.astype(jnp.bfloat16)).astype(jnp.float32)
        block_num = jnp.einsum('bhp,bphv->bhv', block_prob, value_block)
        return (block_max, block_den, block_num)
    block_ids = jnp.arange(CACHE_CAPACITY // POS_DEV, dtype=jnp.int32)
    block_maxes, block_dens, block_nums = lax.map(one_block, block_ids)
    cache_max = lax.optimization_barrier(jnp.max(block_maxes, axis=0))
    rescale = jnp.exp(block_maxes - cache_max[None])
    cache_den = lax.optimization_barrier(jnp.sum(rescale * block_dens, axis=0))
    cache_num = lax.optimization_barrier(jnp.sum(rescale[..., None] * block_nums, axis=0))
    last_index = jnp.broadcast_to((lengths - 1).astype(jnp.int32)[:, None, None], (BATCH_SEQUENCES, HEAD_COUNT, 1))
    carried = jnp.take_along_axis(cache_fcum, last_index, axis=2)[:, :, 0] + log_forget
    own_score = lax.optimization_barrier(jnp.sum(query_f32 * new_key.astype(jnp.float32), axis=2)) * inv_root
    own_prob = lax.optimization_barrier(own_score.astype(jnp.bfloat16)).astype(jnp.float32)
    own_num = own_prob[..., None] * new_value.astype(jnp.float32)
    highest = jnp.maximum(carried + cache_max, in_gate)
    weight_cache = jnp.exp(carried + cache_max - highest)
    weight_own = jnp.exp(in_gate - highest)
    denominator = weight_cache * cache_den + weight_own * own_score
    numerator = weight_cache[..., None] * cache_num + weight_own[..., None] * own_num
    heads_out = (numerator / jnp.maximum(jnp.abs(denominator), 1.0)[..., None]).astype(jnp.bfloat16).reshape(BATCH_SEQUENCES, HEAD_COUNT * V)
    residual = (token_f32 + jnp.dot(heads_out, w_out, preferred_element_type=jnp.float32)).astype(jnp.bfloat16)
    resid_f32 = residual.astype(jnp.float32)
    inv_norm_ffn = lax.rsqrt(lax.optimization_barrier(jnp.mean(resid_f32 * resid_f32, axis=1, keepdims=True)) + epsilon)
    normed = (resid_f32 * inv_norm_ffn * gain_ffn.astype(jnp.float32)[None, :]).astype(jnp.bfloat16)
    gate_act = jnp.dot(normed, w_gate, preferred_element_type=jnp.float32)
    up_act = jnp.dot(normed, w_up, preferred_element_type=jnp.float32)
    hidden = (jax.nn.silu(gate_act) * up_act).astype(jnp.bfloat16)
    return (resid_f32 + jnp.dot(hidden, w_down, preferred_element_type=jnp.float32)).astype(jnp.bfloat16)
```

```python
import functools

import jax
import jax.numpy as jnp
from jax import lax
from jax.experimental import pallas as pl
from jax.experimental.pallas import tpu as pltpu
from jax.sharding import PartitionSpec as P

epsilon = 1e-06
very_low = -1e30


def combined_all(value, axis, join):
    pieces = jax.tree.map(lambda part: lax.all_gather(part, axis), value)
    head = jax.tree.map(lambda part: part[0], pieces)
    tail = jax.tree.map(lambda part: part[1:], pieces)
    total, _ = lax.scan(lambda total, piece: (join(total, piece), None), head, tail)
    return total


def merge_partial(first_part, second_part):
    max_first, den_first, num_first, anchor_first = first_part
    max_second, den_second, num_second, anchor_second = second_part
    highest = jnp.maximum(max_first, max_second)
    scale_first = jnp.exp(max_first - highest)
    scale_second = jnp.exp(max_second - highest)
    denominator = scale_first * den_first + scale_second * den_second
    numerator = scale_first[..., None] * num_first + scale_second[..., None] * num_second
    return (highest, denominator, numerator, jnp.maximum(anchor_first, anchor_second))


def per_device(
    tokens,
    lengths,
    cache_keys,
    cache_values,
    cache_igate,
    cache_fcum,
    gain_mix,
    w_query,
    w_key,
    w_value,
    w_gates,
    w_out,
    gain_ffn,
    w_gate,
    w_up,
    w_down,
):
    count_dp = lax.axis_size("dp")
    count_kv = lax.axis_size("kv")
    count_tp = lax.axis_size("tp")
    index_dp = lax.axis_index("dp")
    index_kv = lax.axis_index("kv")
    index_tp = lax.axis_index("tp")
    row_count, feat_block = tokens.shape
    seq_count, block_len, head_local, key_dimension = cache_keys.shape
    value_size = cache_values.shape[3]
    model_width = gain_mix.shape[0]
    heads_total = w_gates.shape[1] // 2
    out_block = w_out.shape[1]
    col_start = (index_dp * count_kv + index_kv) * feat_block
    token_f32 = tokens.astype(jnp.float32)
    gain_part = lax.dynamic_slice_in_dim(gain_mix, col_start, feat_block, 0).astype(jnp.float32)
    scaled = (token_f32 * gain_part[None, :]).astype(jnp.bfloat16)
    energy = jnp.sum(token_f32 * token_f32, axis=1)
    joined = jnp.concatenate(
        [
            jnp.dot(scaled, w_query, preferred_element_type=jnp.float32),
            jnp.dot(scaled, w_key, preferred_element_type=jnp.float32),
            jnp.dot(scaled, w_value, preferred_element_type=jnp.float32),
        ],
        axis=1,
    )
    gate_rows = lax.dynamic_slice_in_dim(w_gates, col_start, feat_block, 0).reshape(
        feat_block, 2, heads_total
    )
    gate_cols = lax.dynamic_slice_in_dim(gate_rows, index_tp * head_local, head_local, 2).reshape(
        feat_block, 2 * head_local
    )
    gate_part = jnp.dot(scaled, gate_cols, preferred_element_type=jnp.float32)
    joined_part, gate_rowsum, energy_part = (
        lax.psum_scatter(joined, "dp", scatter_dimension=0, tiled=True),
        lax.psum_scatter(gate_part, "dp", scatter_dimension=0, tiled=True),
        lax.psum_scatter(energy, "dp", scatter_dimension=0, tiled=True),
    )
    joined_own, gate_own, energy_own = lax.psum((joined_part, gate_rowsum, energy_part), "kv")
    inv_norm = lax.rsqrt(energy_own / model_width + epsilon)[:, None]
    width_qk = head_local * key_dimension
    query_new = (
        (joined_own[:, :width_qk] * inv_norm)
        .astype(jnp.bfloat16)
        .reshape(seq_count, head_local, key_dimension)
    )
    new_key = (
        (joined_own[:, width_qk : 2 * width_qk] * inv_norm)
        .astype(jnp.bfloat16)
        .reshape(seq_count, head_local, key_dimension)
    )
    new_value = (
        (joined_own[:, 2 * width_qk :] * inv_norm)
        .astype(jnp.bfloat16)
        .reshape(seq_count, head_local, value_size)
    )
    gates_now = gate_own * inv_norm
    in_gate = gates_now[:, :head_local]
    log_forget = jax.nn.log_sigmoid(gates_now[:, head_local:])
    inv_root = key_dimension ** (-0.5)
    scores = (
        jnp.einsum("shk,sphk->shp", query_new, cache_keys, preferred_element_type=jnp.float32)
        * inv_root
    )
    positions = index_kv * block_len + jnp.arange(block_len, dtype=jnp.int32)
    is_live = positions[None, None, :] < lengths[:, None, None]
    exponent = jnp.where(is_live, cache_igate - cache_fcum, very_low)
    block_max = jnp.max(exponent, axis=2)
    weight = jnp.where(is_live, jnp.exp(exponent - block_max[..., None]), 0.0)
    product = weight * scores
    block_den = jnp.sum(product, axis=2)
    block_num = jnp.einsum(
        "shp,sphv->shv",
        product.astype(jnp.bfloat16),
        cache_values,
        preferred_element_type=jnp.float32,
    )
    holding = positions[None, None, :] == (lengths - 1)[:, None, None]
    anchor = jnp.max(jnp.where(holding, cache_fcum, very_low), axis=2)
    cache_max, cache_den, cache_num, anchor_all = combined_all(
        (block_max, block_den, block_num, anchor), "kv", merge_partial
    )
    own_score = (
        jnp.sum(query_new.astype(jnp.float32) * new_key.astype(jnp.float32), axis=2) * inv_root
    )
    own_prob = lax.optimization_barrier(own_score.astype(jnp.bfloat16)).astype(jnp.float32)
    own_num = own_prob[..., None] * new_value.astype(jnp.float32)
    carried = anchor_all + log_forget
    highest = jnp.maximum(carried + cache_max, in_gate)
    weight_cache = jnp.exp(carried + cache_max - highest)
    weight_own = jnp.exp(in_gate - highest)
    denominator = weight_cache * cache_den + weight_own * own_score
    numerator = weight_cache[..., None] * cache_num + weight_own[..., None] * own_num
    heads_out = (numerator / jnp.maximum(jnp.abs(denominator), 1.0)[..., None]).astype(jnp.bfloat16)
    heads_out = heads_out.reshape(seq_count, head_local * value_size)
    gathered = lax.all_gather(heads_out[None], ("dp", "tp"), axis=0, tiled=True)
    gathered = gathered.reshape(count_dp, count_tp, seq_count, head_local * value_size)
    out_weight = w_out.reshape(count_tp, head_local * value_size, out_block)
    attended = jnp.einsum(
        "atsk,tkc->asc", gathered, out_weight, preferred_element_type=jnp.float32
    ).reshape(row_count, out_block)
    own_cols = lax.dynamic_slice_in_dim(token_f32, index_tp * out_block, out_block, 1)
    residual = (own_cols + attended).astype(jnp.bfloat16)
    full_rows = lax.all_gather(residual, ("dp", "kv", "tp"), axis=1, tiled=True)
    full_f32 = full_rows.astype(jnp.float32)
    inv_norm_ffn = lax.rsqrt(jnp.mean(full_f32 * full_f32, axis=1, keepdims=True) + epsilon)
    normed = (full_f32 * inv_norm_ffn * gain_ffn.astype(jnp.float32)[None, :]).astype(jnp.bfloat16)
    gate_act = jnp.dot(normed, w_gate, preferred_element_type=jnp.float32)
    up_act = jnp.dot(normed, w_up, preferred_element_type=jnp.float32)
    hidden = (jax.nn.silu(gate_act) * up_act).astype(jnp.bfloat16)
    summed = lax.psum_scatter(
        lax.dot_general(
            w_down, hidden, (((0,), (1,)), ((), ())), preferred_element_type=jnp.float32
        ),
        ("dp", "kv", "tp"),
        scatter_dimension=0,
        tiled=True,
    )
    return (residual.astype(jnp.float32) + summed.T).astype(jnp.bfloat16)


def fused_kernel(
    sizes, lengths, tokens, cache_igate, cache_fcum, gain_mix, gain_ffn,
    cache_keys, cache_values, w_query, w_key, w_value, w_gates, w_out, w_gate, w_up, w_down,
    out_ref,
    len_s, tok_v, igate_v, fcum_v, gain_raw,
    wq_v, wk_v, wv_v, wg_v, wo_v, wgate_v, wup_v, wdown_v,
    keys_v, values_v,
    q_src, kv_src, small_src, q_rx, kv_rx, small_rx,
    part_src, part_rx, heads_rx, resid_rx, down_src, down_rx, gains,
    load_sem, send_sem, recv_sem,
):
    count_dp, count_kv, count_tp = sizes
    count = count_dp * count_kv * count_tp
    blocks = count_dp * count_kv
    dp, kv, tp = lax.axis_index("dp"), lax.axis_index("kv"), lax.axis_index("tp")
    f32, bf16 = jnp.float32, jnp.bfloat16
    seqs, heads, block_len, key_size = cache_keys.shape
    value_size = cache_values.shape[3]
    rows, feat = tokens.shape
    width_q = heads * key_size
    width_v = heads * value_size
    half_kv = (width_q + width_v) // 2
    out_block = out_ref.shape[1]
    model_width = feat * blocks
    heads_total = heads * count_tp
    block = dp * count_kv + kv
    me = block * count_tp + tp

    def split(r):
        return r // (count_kv * count_tp), (r // count_tp) % count_kv, r % count_tp

    def target(r):
        a, b, c = split(r)
        return dp ^ a, kv ^ b, tp ^ c

    def place(r):
        t = target(r)
        return (t[0] * count_kv + t[1]) * count_tp + t[2]

    def device(r):
        t = target(r)
        return {"dp": t[0], "kv": t[1], "tp": t[2]}

    def distance(r):
        a, b, c = split(r)
        return (a + b) * 2 + c

    near = sorted(range(1, count), key=distance)
    peers = sorted(range(count_tp, count, count_tp), key=distance)[::-1]

    def gain_row(which, at, width):
        lines = width // 128
        first = at * lines
        return jnp.concatenate(
            [gains[which, pl.ds(first + i, 1), :] for i in range(lines)], axis=1
        )

    def load(hbm, vmem, index, pieces=1):
        step = hbm.shape[0] // pieces
        for i in range(pieces):
            pltpu.make_async_copy(
                hbm.at[pl.ds(i * step, step)], vmem.at[pl.ds(i * step, step)], load_sem.at[index]
            ).start()

    def loaded(vmem, index):
        pltpu.make_async_copy(vmem, vmem, load_sem.at[index]).wait()

    def remote(src, dst, send, recv, r):
        pltpu.make_async_remote_copy(
            src_ref=src, dst_ref=dst, send_sem=send_sem.at[send], recv_sem=recv_sem.at[recv],
            device_id=device(r), device_id_type=pl.DeviceIdType.MESH,
        ).start()

    def arrived(like, recv):
        pltpu.make_async_copy(like, like, recv_sem.at[recv]).wait()

    def sent(like, send):
        pltpu.make_async_copy(like, like, send_sem.at[send]).wait()

    barrier = pltpu.get_barrier_semaphore()
    for r in near[::-1]:
        pl.semaphore_signal(
            barrier, inc=1, device_id=device(r), device_id_type=pl.DeviceIdType.MESH
        )
    load(tokens, tok_v, 0)
    load(gain_mix, gain_raw.at[0], 1)
    gate_start = pl.multiple_of(block * feat, feat)
    pltpu.make_async_copy(w_gates.at[:, pl.ds(gate_start, feat)], wg_v, load_sem.at[3]).start()
    load(w_query, wq_v, 4, 4)
    load(lengths, len_s, 2)
    load(cache_igate, igate_v, 5)
    load(cache_fcum, fcum_v, 6)
    load(w_key, wk_v, 7, 2)
    load(w_value, wv_v, 8, 4)

    dot = functools.partial(jnp.dot, preferred_element_type=f32)
    loaded(tok_v, 0)
    loaded(gain_raw.at[0], 1)
    gains[0] = gain_raw[0].astype(f32)
    token = tok_v[...].astype(f32)
    scaled = (token * gain_row(0, block, feat)).astype(bf16)
    energy = jnp.sum(token * token, axis=1, keepdims=True)
    loaded(wg_v, 3)
    gate_part = lax.dot_general(
        scaled, wg_v[...], (((1,), (1,)), ((), ())), preferred_element_type=f32
    )
    gate_part = jnp.concatenate(
        [gate_part, jnp.zeros((rows, 128 - 2 * heads_total), f32)], axis=1
    )
    shifted = gate_part
    for c in range(1, count_tp):
        shifted = jnp.where(tp == c, pltpu.roll(gate_part, 128 - c * heads, 1), shifted)
    lane_all = lax.broadcasted_iota(jnp.int32, (rows, 128), 1)
    at_energy, at_max, at_anchor = 16, 32, 64
    shifted = jnp.where(lane_all == at_energy, energy, shifted)

    loaded(len_s, 2)
    loaded(igate_v, 5)
    loaded(fcum_v, 6)
    lane = lax.broadcasted_iota(jnp.int32, (seqs, 128), 1)
    row = lax.broadcasted_iota(jnp.int32, (seqs, block_len), 0)
    row_v = lax.broadcasted_iota(jnp.int32, (seqs, value_size), 0)
    length = jnp.zeros((seqs, block_len), jnp.int32)
    for s in range(seqs):
        length = jnp.where(row == s, len_s[s], length)
    position = kv * block_len + lax.broadcasted_iota(jnp.int32, (seqs, block_len), 1)
    live = position < length
    holding = position == length - 1
    exponents = []
    stats = jnp.full((seqs, 128), very_low, f32)
    for h in range(heads):
        fcum = fcum_v[h]
        exponent = jnp.where(live, igate_v[h] - fcum, very_low)
        exponents.append(exponent)
        top = jnp.max(exponent, axis=1, keepdims=True)
        anchor = jnp.max(jnp.where(holding, fcum, very_low), axis=1, keepdims=True)
        stats = jnp.where(lane == at_max + h, top, stats)
        stats = jnp.where(lane == at_anchor + h, anchor, stats)
    for a in range(count_dp):
        part = shifted[a * seqs : (a + 1) * seqs]
        small_src[a] = jnp.where(lane < at_max, part, stats)

    loaded(wq_v, 4)
    query = dot(scaled, wq_v[...])
    for a in range(count_dp):
        q_src[a] = query[a * seqs : (a + 1) * seqs].astype(bf16)
    pl.semaphore_wait(barrier, count - 1)
    for r in peers:
        n, to = r // count_tp, target(r)[0]
        remote(small_src.at[to], small_rx.at[n], 0, 0, r)
        remote(q_src.at[to], q_rx.at[n], 1, 1, r)
    for s in range(seqs):
        span = pl.ds(s * block_len, block_len)
        pltpu.make_async_copy(cache_keys.at[s], keys_v.at[:, span, :], load_sem.at[9]).start()
    for s in range(seqs):
        span = pl.ds(s * block_len, block_len)
        pltpu.make_async_copy(cache_values.at[s], values_v.at[:, span, :], load_sem.at[10]).start()
    loaded(wk_v, 7)
    key_part = dot(scaled, wk_v[...])
    loaded(wv_v, 8)
    load(w_out, wo_v, 11, 4)
    load(gain_ffn, gain_raw.at[1], 15)
    load(w_gate, wgate_v, 12, 8)
    load(w_up, wup_v, 13, 8)
    for j in range(count):
        pltpu.make_async_copy(
            w_down.at[:, pl.ds(j * out_block, out_block)], wdown_v.at[j], load_sem.at[14]
        ).start()
    value_part = dot(scaled, wv_v[...])
    joined = jnp.concatenate([key_part, value_part], axis=1)
    for i in range(rows):
        line = joined[i : i + 1]
        kv_src[i] = jnp.concatenate([line[:, :half_kv], line[:, half_kv:]], axis=0).astype(bf16)
    for r in peers:
        t = target(r)
        remote(kv_src.at[t[0] * count_kv + t[1]], kv_rx.at[r // count_tp], 2, 2, r)

    arrived(small_rx.at[pl.ds(1, blocks - 1)], 0)
    small = small_src[dp]
    extreme = small
    for n in range(1, blocks):
        small += small_rx[n]
        if n < count_kv:
            extreme = jnp.maximum(extreme, small_rx[n])
    inv_norm = lax.rsqrt(small[:, at_energy : at_energy + 1] / model_width + epsilon)
    gates_now = small * inv_norm
    log_forget = jnp.minimum(gates_now, 0.0) - jnp.log1p(jnp.exp(-jnp.abs(gates_now)))
    forget_here = pltpu.roll(log_forget, 128 - heads_total, 1)
    top_here = pltpu.roll(extreme, 128 - at_max, 1)
    carried = pltpu.roll(extreme, 128 - at_anchor, 1) + forget_here
    highest = jnp.maximum(carried + top_here, gates_now)
    offset = carried - highest
    own_weight = jnp.exp(gates_now - highest)
    weights = []
    for h in range(heads):
        power = jnp.where(live, exponents[h] + offset[:, h : h + 1], very_low)
        weights.append(jnp.where(live, jnp.exp(power), 0.0))

    arrived(q_rx.at[pl.ds(1, blocks - 1)], 1)
    q_total = q_src[dp].astype(f32)
    for n in range(1, blocks):
        q_total += q_rx[n].astype(f32)
    query_new = (q_total * inv_norm).astype(bf16)
    loaded(keys_v, 9)
    inv_root = key_size ** (-0.5)
    probs, dens, nums = [], [], []
    for h in range(heads):
        found = lax.dot_general(
            query_new[:, h * key_size : (h + 1) * key_size], keys_v[h],
            (((1,), (1,)), ((), ())), preferred_element_type=f32,
        )
        score = found[:, 0:block_len]
        for s in range(1, seqs):
            score = jnp.where(row == s, found[:, s * block_len : (s + 1) * block_len], score)
        product = weights[h] * (score * inv_root)
        dens.append(jnp.sum(product, axis=1, keepdims=True))
        probs.append(
            jnp.concatenate([jnp.where(row == s, product, 0.0) for s in range(seqs)], axis=1).astype(bf16)
        )
    loaded(values_v, 10)
    for h in range(heads):
        nums.append(dot(probs[h], values_v[h]))

    arrived(kv_rx.at[pl.ds(1, blocks - 1)], 2)
    kv_total = kv_src[block].astype(f32)
    for n in range(1, blocks):
        kv_total += kv_rx[n].astype(f32)
    kv_row = jnp.concatenate([kv_total[0:1], kv_total[1:2]], axis=1)
    kv_row = (jnp.broadcast_to(kv_row, (seqs, 2 * half_kv)) * inv_norm).astype(bf16).astype(f32)
    query_f32 = query_new.astype(f32)
    mine = lax.broadcasted_iota(jnp.int32, (seqs, 1), 0) == kv
    den_line = jnp.zeros((seqs, 128), f32)
    for h in range(heads):
        key_h = kv_row[:, h * key_size : (h + 1) * key_size]
        value_h = kv_row[:, width_q + h * value_size : width_q + (h + 1) * value_size]
        query_h = query_f32[:, h * key_size : (h + 1) * key_size]
        score = jnp.sum(query_h * key_h, axis=1, keepdims=True) * inv_root
        own = jnp.where(mine, own_weight[:, h : h + 1], 0.0)
        dens[h] += own * score
        nums[h] += (own * score.astype(bf16).astype(f32)) * value_h
        coarse = dens[h].astype(bf16).astype(f32)
        den_line = jnp.where(lane == h, coarse, den_line)
        den_line = jnp.where(lane == heads + h, dens[h] - coarse, den_line)
        part_src[:, h * value_size : (h + 1) * value_size] = nums[h].astype(bf16)
    part_src[:, width_v : width_v + 128] = den_line.astype(bf16)
    for b in range(count_kv - 1, 0, -1):
        remote(part_src, part_rx.at[b], 3, 3, b * count_tp)

    if count_kv > 1:
        arrived(part_rx.at[pl.ds(1, count_kv - 1)], 3)
    tail = part_rx[1, :, width_v : width_v + 128].astype(f32)
    for b in range(2, count_kv):
        tail += part_rx[b, :, width_v : width_v + 128].astype(f32)
    for h in range(heads):
        span = pl.ds(h * value_size, value_size)
        num = nums[h]
        for b in range(1, count_kv):
            num += part_rx[b, :, span].astype(f32)
        den = dens[h] + tail[:, h : h + 1] + tail[:, heads + h : heads + h + 1]
        heads_rx[dp * count_tp + tp, :, span] = (num / jnp.maximum(jnp.abs(den), 1.0)).astype(bf16)
    d_peers = [r for r in near[::-1] if split(r)[1] == 0]
    for r in d_peers:
        remote(heads_rx.at[dp * count_tp + tp], heads_rx.at[dp * count_tp + tp], 4, 4, r)
    loaded(wo_v, 11)
    loaded(gain_raw.at[1], 15)
    gains[1] = gain_raw[1].astype(f32)
    arrived(heads_rx.at[pl.ds(0, len(d_peers))], 4)
    lines = [
        jnp.concatenate([heads_rx[a * count_tp + c].astype(f32) for c in range(count_tp)], axis=1)
        for a in range(count_dp)
    ]
    attended = dot(jnp.concatenate(lines, axis=0).astype(bf16), wo_v[...])
    own_cols = tok_v[:, pl.ds(pl.multiple_of(tp * out_block, out_block), out_block)].astype(f32)
    residual = (own_cols + attended).astype(bf16)
    resid_rx[me] = residual
    levels = sorted({distance(r) // 2 for r in range(count)})
    groups = [[r for r in [0] + near if distance(r) // 2 == level] for level in levels]
    which = {r: i for i, group in enumerate(groups) for r in group}
    for r in near[::-1]:
        remote(resid_rx.at[me], resid_rx.at[me], 5, 5 + which[r], r)
    loaded(wgate_v, 12)
    loaded(wup_v, 13)
    gate_act = up_act = square = 0.0
    for i, group in enumerate(groups):
        others = sum(r > 0 for r in group)
        arrived(resid_rx.at[pl.ds(0, others)], 5 + i)
        for r in group:
            at = place(r)
            piece = resid_rx[at].astype(f32) if r else residual.astype(f32)
            square += jnp.sum(piece * piece, axis=1, keepdims=True)
            piece = (piece * gain_row(1, at, out_block)).astype(bf16)
            span = pl.ds(pl.multiple_of(at * out_block, out_block), out_block)
            gate_act += dot(piece, wgate_v[span, :])
            up_act += dot(piece, wup_v[span, :])
    inv_ffn = lax.rsqrt(square / model_width + epsilon)
    gate_act = gate_act * inv_ffn
    up_act = up_act * inv_ffn
    hidden = (gate_act / (1.0 + jnp.exp(-gate_act)) * up_act).astype(bf16)
    loaded(wdown_v, 14)
    last = 5 + len(groups)
    order = near[::-1]
    for first in range(0, count - 1, 2):
        pair = order[first : first + 2]
        for r in pair:
            down_src[r] = dot(hidden, wdown_v[place(r)]).astype(bf16)
        for r in pair:
            remote(down_src.at[r], down_rx.at[r], 6, last, r)
    total = residual.astype(f32) + dot(hidden, wdown_v[me])
    sent(small_rx.at[pl.ds(1, blocks - 1)], 0)
    sent(q_rx.at[pl.ds(1, blocks - 1)], 1)
    sent(kv_rx.at[pl.ds(1, blocks - 1)], 2)
    if count_kv > 1:
        sent(part_rx.at[pl.ds(1, count_kv - 1)], 3)
    sent(heads_rx.at[pl.ds(0, len(d_peers))], 4)
    sent(resid_rx.at[pl.ds(0, count - 1)], 5)
    arrived(down_rx.at[pl.ds(1, count - 1)], last)
    for r in near:
        total += down_rx[r].astype(f32)
    out_ref[...] = total.astype(bf16)
    sent(down_rx.at[pl.ds(1, count - 1)], 6)


def fused(
    tokens, lengths, cache_keys, cache_values, cache_igate, cache_fcum, gain_mix,
    w_query, w_key, w_value, w_gates, w_out, gain_ffn, w_gate, w_up, w_down,
):
    sizes = tuple(lax.axis_size(name) for name in ("dp", "kv", "tp"))
    count = sizes[0] * sizes[1] * sizes[2]
    blocks = sizes[0] * sizes[1]
    f32, bf16 = jnp.float32, jnp.bfloat16
    rows, feat = tokens.shape
    seqs, block_len, heads, key_size = cache_keys.shape
    value_size = cache_values.shape[3]
    out_block = w_out.shape[1]
    half_kv = heads * (key_size + value_size) // 2
    width_v = heads * value_size
    hbm = pl.BlockSpec(memory_space=pl.ANY)
    vmem = pl.BlockSpec(memory_space=pltpu.VMEM)
    dma = pltpu.SemaphoreType.DMA
    scratch = [
        pltpu.SMEM((seqs,), jnp.int32),
        pltpu.VMEM(tokens.shape, bf16),
        pltpu.VMEM((heads, seqs, block_len), f32),
        pltpu.VMEM((heads, seqs, block_len), f32),
        pltpu.VMEM((2, blocks * feat // 128, 128), bf16),
        pltpu.VMEM(w_query.shape, bf16),
        pltpu.VMEM(w_key.shape, bf16),
        pltpu.VMEM(w_value.shape, bf16),
        pltpu.VMEM((w_gates.shape[1], feat), bf16),
        pltpu.VMEM(w_out.shape, bf16),
        pltpu.VMEM(w_gate.shape, bf16),
        pltpu.VMEM(w_up.shape, bf16),
        pltpu.VMEM((count, w_down.shape[0], out_block), bf16),
        pltpu.VMEM((heads, seqs * block_len, key_size), bf16),
        pltpu.VMEM((heads, seqs * block_len, value_size), bf16),
        pltpu.VMEM((sizes[0], seqs, heads * key_size), bf16),
        pltpu.VMEM((rows, 2, half_kv), bf16),
        pltpu.VMEM((sizes[0], seqs, 128), f32),
        pltpu.VMEM((blocks, seqs, heads * key_size), bf16),
        pltpu.VMEM((blocks, 2, half_kv), bf16),
        pltpu.VMEM((blocks, seqs, 128), f32),
        pltpu.VMEM((seqs, width_v + 128), bf16),
        pltpu.VMEM((sizes[1], seqs, width_v + 128), bf16),
        pltpu.VMEM((sizes[0] * sizes[2], seqs, width_v), bf16),
        pltpu.VMEM((count, rows, out_block), bf16),
        pltpu.VMEM((count, rows, out_block), bf16),
        pltpu.VMEM((count, rows, out_block), bf16),
        pltpu.VMEM((2, blocks * feat // 128, 128), f32),
        dma((16,)),
        dma((7,)),
        dma((6 + 5,)),
    ]
    operands = (
        lengths, tokens, cache_igate.swapaxes(0, 1), cache_fcum.swapaxes(0, 1),
        gain_mix.reshape(-1, 128), gain_ffn.reshape(-1, 128),
        cache_keys.swapaxes(1, 2), cache_values.swapaxes(1, 2),
        w_query, w_key, w_value, w_gates.T, w_out, w_gate, w_up, w_down,
    )
    return pl.pallas_call(
        functools.partial(fused_kernel, sizes),
        out_shape=pltpu.VMEM((rows, out_block), bf16),
        in_specs=[hbm] * len(operands),
        out_specs=vmem,
        scratch_shapes=scratch,
        compiler_params=pltpu.CompilerParams(
            collective_id=0, has_side_effects=True, vmem_limit_bytes=40 * 1024 * 1024
        ),
    )(*[pltpu.with_memory_space_constraint(x, pltpu.HBM) for x in operands])


def fits_kernel(tokens, cache_keys, w_out, w_gate):
    return (
        cache_keys.shape[0] == lax.axis_size("kv")
        and all(n in (2, 4) for n in map(lax.axis_size, ("dp", "kv", "tp")))
        and cache_keys.shape[2] <= 4
        and tokens.shape[1] % 128 == 0
        and w_out.shape[1] % 128 == 0
        and w_gate.shape[1] % 128 == 0
    )


def layer(*args):
    if fits_kernel(args[0], args[2], args[11], args[13]):
        return fused(*args)
    return per_device(*args)


def solution(mesh):
    in_specs = (
        P("grp", ("dp", "kv")),
        P(("grp", "dp")),
        P(("grp", "dp"), "kv", "tp", None),
        P(("grp", "dp"), "kv", "tp", None),
        P(("grp", "dp"), "tp", "kv"),
        P(("grp", "dp"), "tp", "kv"),
        P(),
        P(("dp", "kv"), "tp"),
        P(("dp", "kv"), "tp"),
        P(("dp", "kv"), "tp"),
        P(),
        P(None, ("dp", "kv", "tp")),
        P(),
        P(None, ("dp", "kv", "tp")),
        P(None, ("dp", "kv", "tp")),
        P(("dp", "kv", "tp"), None),
    )
    out_specs = P("grp", ("dp", "kv", "tp"))
    return jax.shard_map(
        layer, mesh=mesh, in_specs=in_specs, out_specs=out_specs, check_vma=False
    )
```

```python
import functools

import jax
import jax.numpy as jnp
from jax import lax
from jax.experimental import pallas as pl
from jax.experimental.pallas import tpu as pltpu
from jax.sharding import PartitionSpec as P

epsilon = 1e-06
very_low = -1e30


def combined_all(value, axis, join):
    pieces = jax.tree.map(lambda part: lax.all_gather(part, axis), value)
    head = jax.tree.map(lambda part: part[0], pieces)
    tail = jax.tree.map(lambda part: part[1:], pieces)
    total, _ = lax.scan(lambda total, piece: (join(total, piece), None), head, tail)
    return total


def merge_partial(first_part, second_part):
    max_first, den_first, num_first, anchor_first = first_part
    max_second, den_second, num_second, anchor_second = second_part
    highest = jnp.maximum(max_first, max_second)
    scale_first = jnp.exp(max_first - highest)
    scale_second = jnp.exp(max_second - highest)
    denominator = scale_first * den_first + scale_second * den_second
    numerator = scale_first[..., None] * num_first + scale_second[..., None] * num_second
    return (highest, denominator, numerator, jnp.maximum(anchor_first, anchor_second))


def per_device(
    tokens,
    lengths,
    cache_keys,
    cache_values,
    cache_igate,
    cache_fcum,
    gain_mix,
    w_query,
    w_key,
    w_value,
    w_gates,
    w_out,
    gain_ffn,
    w_gate,
    w_up,
    w_down,
):
    count_dp = lax.axis_size("dp")
    count_kv = lax.axis_size("kv")
    count_tp = lax.axis_size("tp")
    index_dp = lax.axis_index("dp")
    index_kv = lax.axis_index("kv")
    index_tp = lax.axis_index("tp")
    row_count, feat_block = tokens.shape
    seq_count, block_len, head_local, key_dimension = cache_keys.shape
    value_size = cache_values.shape[3]
    model_width = gain_mix.shape[0]
    heads_total = w_gates.shape[1] // 2
    out_block = w_out.shape[1]
    col_start = (index_dp * count_kv + index_kv) * feat_block
    token_f32 = tokens.astype(jnp.float32)
    gain_part = lax.dynamic_slice_in_dim(gain_mix, col_start, feat_block, 0).astype(jnp.float32)
    scaled = (token_f32 * gain_part[None, :]).astype(jnp.bfloat16)
    energy = jnp.sum(token_f32 * token_f32, axis=1)
    joined = jnp.concatenate(
        [
            jnp.dot(scaled, w_query, preferred_element_type=jnp.float32),
            jnp.dot(scaled, w_key, preferred_element_type=jnp.float32),
            jnp.dot(scaled, w_value, preferred_element_type=jnp.float32),
        ],
        axis=1,
    )
    gate_rows = lax.dynamic_slice_in_dim(w_gates, col_start, feat_block, 0).reshape(
        feat_block, 2, heads_total
    )
    gate_cols = lax.dynamic_slice_in_dim(gate_rows, index_tp * head_local, head_local, 2).reshape(
        feat_block, 2 * head_local
    )
    gate_part = jnp.dot(scaled, gate_cols, preferred_element_type=jnp.float32)
    joined_part, gate_rowsum, energy_part = (
        lax.psum_scatter(joined, "dp", scatter_dimension=0, tiled=True),
        lax.psum_scatter(gate_part, "dp", scatter_dimension=0, tiled=True),
        lax.psum_scatter(energy, "dp", scatter_dimension=0, tiled=True),
    )
    joined_own, gate_own, energy_own = lax.psum((joined_part, gate_rowsum, energy_part), "kv")
    inv_norm = lax.rsqrt(energy_own / model_width + epsilon)[:, None]
    width_qk = head_local * key_dimension
    query_new = (
        (joined_own[:, :width_qk] * inv_norm)
        .astype(jnp.bfloat16)
        .reshape(seq_count, head_local, key_dimension)
    )
    new_key = (
        (joined_own[:, width_qk : 2 * width_qk] * inv_norm)
        .astype(jnp.bfloat16)
        .reshape(seq_count, head_local, key_dimension)
    )
    new_value = (
        (joined_own[:, 2 * width_qk :] * inv_norm)
        .astype(jnp.bfloat16)
        .reshape(seq_count, head_local, value_size)
    )
    gates_now = gate_own * inv_norm
    in_gate = gates_now[:, :head_local]
    log_forget = jax.nn.log_sigmoid(gates_now[:, head_local:])
    inv_root = key_dimension ** (-0.5)
    scores = (
        jnp.einsum("shk,sphk->shp", query_new, cache_keys, preferred_element_type=jnp.float32)
        * inv_root
    )
    positions = index_kv * block_len + jnp.arange(block_len, dtype=jnp.int32)
    is_live = positions[None, None, :] < lengths[:, None, None]
    exponent = jnp.where(is_live, cache_igate - cache_fcum, very_low)
    block_max = jnp.max(exponent, axis=2)
    weight = jnp.where(is_live, jnp.exp(exponent - block_max[..., None]), 0.0)
    product = weight * scores
    block_den = jnp.sum(product, axis=2)
    block_num = jnp.einsum(
        "shp,sphv->shv",
        product.astype(jnp.bfloat16),
        cache_values,
        preferred_element_type=jnp.float32,
    )
    holding = positions[None, None, :] == (lengths - 1)[:, None, None]
    anchor = jnp.max(jnp.where(holding, cache_fcum, very_low), axis=2)
    cache_max, cache_den, cache_num, anchor_all = combined_all(
        (block_max, block_den, block_num, anchor), "kv", merge_partial
    )
    own_score = (
        jnp.sum(query_new.astype(jnp.float32) * new_key.astype(jnp.float32), axis=2) * inv_root
    )
    own_prob = lax.optimization_barrier(own_score.astype(jnp.bfloat16)).astype(jnp.float32)
    own_num = own_prob[..., None] * new_value.astype(jnp.float32)
    carried = anchor_all + log_forget
    highest = jnp.maximum(carried + cache_max, in_gate)
    weight_cache = jnp.exp(carried + cache_max - highest)
    weight_own = jnp.exp(in_gate - highest)
    denominator = weight_cache * cache_den + weight_own * own_score
    numerator = weight_cache[..., None] * cache_num + weight_own[..., None] * own_num
    heads_out = (numerator / jnp.maximum(jnp.abs(denominator), 1.0)[..., None]).astype(jnp.bfloat16)
    heads_out = heads_out.reshape(seq_count, head_local * value_size)
    gathered = lax.all_gather(heads_out[None], ("dp", "tp"), axis=0, tiled=True)
    gathered = gathered.reshape(count_dp, count_tp, seq_count, head_local * value_size)
    out_weight = w_out.reshape(count_tp, head_local * value_size, out_block)
    attended = jnp.einsum(
        "atsk,tkc->asc", gathered, out_weight, preferred_element_type=jnp.float32
    ).reshape(row_count, out_block)
    own_cols = lax.dynamic_slice_in_dim(token_f32, index_tp * out_block, out_block, 1)
    residual = (own_cols + attended).astype(jnp.bfloat16)
    full_rows = lax.all_gather(residual, ("dp", "kv", "tp"), axis=1, tiled=True)
    full_f32 = full_rows.astype(jnp.float32)
    inv_norm_ffn = lax.rsqrt(jnp.mean(full_f32 * full_f32, axis=1, keepdims=True) + epsilon)
    normed = (full_f32 * inv_norm_ffn * gain_ffn.astype(jnp.float32)[None, :]).astype(jnp.bfloat16)
    gate_act = jnp.dot(normed, w_gate, preferred_element_type=jnp.float32)
    up_act = jnp.dot(normed, w_up, preferred_element_type=jnp.float32)
    hidden = (jax.nn.silu(gate_act) * up_act).astype(jnp.bfloat16)
    summed = lax.psum_scatter(
        lax.dot_general(
            w_down, hidden, (((0,), (1,)), ((), ())), preferred_element_type=jnp.float32
        ),
        ("dp", "kv", "tp"),
        scatter_dimension=0,
        tiled=True,
    )
    return (residual.astype(jnp.float32) + summed.T).astype(jnp.bfloat16)


def fused_kernel(
    sizes, lengths, tokens, cache_igate, cache_fcum, gain_mix, gain_ffn,
    cache_keys, cache_values, w_query, w_key, w_value, w_gates, w_out, w_gate, w_up, w_down,
    out_ref,
    len_s, tok_v, igate_v, fcum_v, gain_raw,
    wq_v, wk_v, wv_v, wg_v, wo_v, wgate_v, wup_v, wdown_v,
    keys_v, values_v,
    keys_t, q_src, kv_src, small_src, q_rx, kv_rx, small_rx,
    own_part, part_src, part_rx, heads_rx, resid_rx, down_src, down_rx, gains,
    load_sem, send_sem, recv_sem,
):
    count_dp, count_kv, count_tp = sizes
    count = count_dp * count_kv * count_tp
    blocks = count_dp * count_kv
    dp, kv, tp = lax.axis_index("dp"), lax.axis_index("kv"), lax.axis_index("tp")
    f32, bf16 = jnp.float32, jnp.bfloat16
    seqs, heads, block_len, key_size = cache_keys.shape
    value_size = cache_values.shape[3]
    rows, feat = tokens.shape
    width_q = heads * key_size
    width_v = heads * value_size
    half_kv = (width_q + width_v) // 2
    out_block = out_ref.shape[1]
    model_width = feat * blocks
    heads_total = heads * count_tp
    block = dp * count_kv + kv
    me = block * count_tp + tp
    lead = count_tp - 1
    leads, follows = tp == lead, tp != lead

    def split(r):
        return r // (count_kv * count_tp), (r // count_tp) % count_kv, r % count_tp

    def target(r):
        a, b, c = split(r)
        return dp ^ a, kv ^ b, tp ^ c

    def place(r):
        t = target(r)
        return (t[0] * count_kv + t[1]) * count_tp + t[2]

    def device(r):
        t = target(r)
        return {"dp": t[0], "kv": t[1], "tp": t[2]}

    def distance(r):
        a, b, c = split(r)
        return (a + b) * 2 + c

    near = sorted(range(1, count), key=distance)
    levels = sorted({distance(r) // 2 for r in range(count)})
    last = 5 + len(levels)
    level_of = {r: levels.index(distance(r) // 2) for r in range(count)}
    peers = sorted(range(count_tp, count, count_tp), key=distance)[::-1]

    def gain_row(which, at, width):
        lines = width // 128
        first = at * lines
        return jnp.concatenate(
            [gains[which, pl.ds(first + i, 1), :] for i in range(lines)], axis=1
        )

    def load(hbm, vmem, index, pieces=1):
        step = hbm.shape[0] // pieces
        for i in range(pieces):
            pltpu.make_async_copy(
                hbm.at[pl.ds(i * step, step)], vmem.at[pl.ds(i * step, step)], load_sem.at[index]
            ).start()

    def loaded(vmem, index):
        pltpu.make_async_copy(vmem, vmem, load_sem.at[index]).wait()

    def remote(src, dst, send, recv, r, core=None):
        where = device(r)
        if core is not None:
            where["tp"] = core
        pltpu.make_async_remote_copy(
            src_ref=src, dst_ref=dst, send_sem=send_sem.at[send], recv_sem=recv_sem.at[recv],
            device_id=where, device_id_type=pl.DeviceIdType.MESH,
        ).start()

    def arrived(like, recv):
        pltpu.make_async_copy(like, like, recv_sem.at[recv]).wait()

    def sent(like, send):
        pltpu.make_async_copy(like, like, send_sem.at[send]).wait()

    barrier = pltpu.get_barrier_semaphore()
    for r in near[::-1]:
        pl.semaphore_signal(
            barrier, inc=1, device_id=device(r), device_id_type=pl.DeviceIdType.MESH
        )
    load(tokens, tok_v, 0)
    load(gain_mix, gain_raw.at[0], 1)
    gate_start = pl.multiple_of(block * feat, feat)
    pltpu.make_async_copy(w_gates.at[:, pl.ds(gate_start, feat)], wg_v, load_sem.at[3]).start()
    load(w_query, wq_v, 4, 4)
    load(lengths, len_s, 2)
    load(cache_igate, igate_v, 5)
    load(cache_fcum, fcum_v, 6)
    load(w_key, wk_v, 7, 2)
    load(w_value, wv_v, 8, 4)

    dot = functools.partial(jnp.dot, preferred_element_type=f32)
    loaded(tok_v, 0)
    loaded(gain_raw.at[0], 1)
    gains[0] = gain_raw[0].astype(f32)
    token = tok_v[...].astype(f32)
    scaled = (token * gain_row(0, block, feat)).astype(bf16)
    energy = jnp.sum(token * token, axis=1, keepdims=True)
    loaded(wg_v, 3)
    gate_part = lax.dot_general(
        scaled, wg_v[...], (((1,), (1,)), ((), ())), preferred_element_type=f32
    )
    gate_part = jnp.concatenate(
        [gate_part, jnp.zeros((rows, 128 - 2 * heads_total), f32)], axis=1
    )
    shifted = gate_part
    for c in range(1, count_tp):
        shifted = jnp.where(tp == c, pltpu.roll(gate_part, 128 - c * heads, 1), shifted)
    lane_all = lax.broadcasted_iota(jnp.int32, (rows, 128), 1)
    at_energy, at_max, at_anchor = 16, 32, 64
    shifted = jnp.where(lane_all == at_energy, energy, shifted)

    loaded(len_s, 2)
    loaded(igate_v, 5)
    loaded(fcum_v, 6)
    lane = lax.broadcasted_iota(jnp.int32, (seqs, 128), 1)
    row = lax.broadcasted_iota(jnp.int32, (seqs, block_len), 0)
    row_v = lax.broadcasted_iota(jnp.int32, (seqs, value_size), 0)
    length = jnp.zeros((seqs, block_len), jnp.int32)
    for s in range(seqs):
        length = jnp.where(row == s, len_s[s], length)
    position = kv * block_len + lax.broadcasted_iota(jnp.int32, (seqs, block_len), 1)
    live = position < length
    holding = position == length - 1
    exponents = []
    stats = jnp.full((seqs, 128), very_low, f32)
    for h in range(heads):
        fcum = fcum_v[h]
        exponent = jnp.where(live, igate_v[h] - fcum, very_low)
        exponents.append(exponent)
        top = jnp.max(exponent, axis=1, keepdims=True)
        anchor = jnp.max(jnp.where(holding, fcum, very_low), axis=1, keepdims=True)
        stats = jnp.where(lane == at_max + h, top, stats)
        stats = jnp.where(lane == at_anchor + h, anchor, stats)
    for a in range(count_dp):
        part = shifted[a * seqs : (a + 1) * seqs]
        small_src[a] = jnp.where(lane < at_max, part, stats)

    loaded(wq_v, 4)
    query = dot(scaled, wq_v[...])
    for a in range(count_dp):
        q_src[a] = query[a * seqs : (a + 1) * seqs].astype(bf16)
    def keys_and_values():
        loaded(wk_v, 7)
        loaded(wv_v, 8)
        joined = jnp.concatenate([dot(scaled, wk_v[...]), dot(scaled, wv_v[...])], axis=1)
        for i in range(rows):
            line = joined[i : i + 1]
            kv_src[i] = jnp.concatenate([line[:, :half_kv], line[:, half_kv:]], axis=0).astype(bf16)

    pl.when(kv == 0)(keys_and_values)
    pl.semaphore_wait(barrier, count - 1)
    for r in peers:
        n, to = r // count_tp, target(r)[0]
        remote(small_src.at[to], small_rx.at[n], 0, 0, r)
        remote(q_src.at[to], q_rx.at[n], 1, 1, r)
    for s in range(seqs):
        span = pl.ds(s * block_len, block_len)
        pltpu.make_async_copy(cache_keys.at[s], keys_v.at[:, span, :], load_sem.at[9]).start()
    for s in range(seqs):
        span = pl.ds(s * block_len, block_len)
        pltpu.make_async_copy(cache_values.at[s], values_v.at[:, span, :], load_sem.at[10]).start()
    pl.when(kv != 0)(keys_and_values)
    for r in peers:
        t = target(r)
        remote(kv_src.at[t[0] * count_kv + t[1]], kv_rx.at[r // count_tp], 2, 2, r)

    @pl.when(follows)
    def _():
        remote(w_out, wo_v.at[tp], 7, last + 1, 0, lead)

    @pl.when(leads)
    def _():
        load(w_out, wo_v.at[lead], 11, 4)

    load(gain_ffn, gain_raw.at[1], 15)
    load(w_gate, wgate_v, 12, 8)
    load(w_up, wup_v, 13, 8)
    for j in range(count):
        pltpu.make_async_copy(
            w_down.at[:, pl.ds(j * out_block, out_block)], wdown_v.at[j], load_sem.at[14]
        ).start()

    loaded(keys_v, 9)
    for h in range(heads):
        keys_t[h] = keys_v[h].T

    arrived(small_rx.at[pl.ds(1, blocks - 1)], 0)
    small = small_src[dp]
    extreme = small
    for n in range(1, blocks):
        small += small_rx[n]
        if n < count_kv:
            extreme = jnp.maximum(extreme, small_rx[n])
    inv_norm = lax.rsqrt(small[:, at_energy : at_energy + 1] / model_width + epsilon)
    gates_now = small * inv_norm
    log_forget = jnp.minimum(gates_now, 0.0) - jnp.log1p(jnp.exp(-jnp.abs(gates_now)))
    forget_here = pltpu.roll(log_forget, 128 - heads_total, 1)
    top_here = pltpu.roll(extreme, 128 - at_max, 1)
    carried = pltpu.roll(extreme, 128 - at_anchor, 1) + forget_here
    highest = jnp.maximum(carried + top_here, gates_now)
    offset = carried - highest
    own_weight = jnp.exp(gates_now - highest)
    weights = []
    for h in range(heads):
        power = jnp.where(live, exponents[h] + offset[:, h : h + 1], very_low)
        weights.append(jnp.where(live, jnp.exp(power), 0.0))

    arrived(q_rx.at[pl.ds(1, blocks - 1)], 1)
    q_total = q_src[dp].astype(f32)
    for n in range(1, blocks):
        q_total += q_rx[n].astype(f32)
    query_new = (q_total * inv_norm).astype(bf16)
    inv_root = key_size ** (-0.5)
    probs, dens, nums = [], [], []
    for h in range(heads):
        found = dot(query_new[:, h * key_size : (h + 1) * key_size], keys_t[h])
        score = found[:, 0:block_len]
        for s in range(1, seqs):
            score = jnp.where(row == s, found[:, s * block_len : (s + 1) * block_len], score)
        product = weights[h] * (score * inv_root)
        dens.append(jnp.sum(product, axis=1, keepdims=True))
        probs.append(
            jnp.concatenate([jnp.where(row == s, product, 0.0) for s in range(seqs)], axis=1).astype(bf16)
        )
    loaded(values_v, 10)
    arrived(kv_rx.at[pl.ds(1, blocks - 1)], 2)
    for h in range(heads):
        nums.append(dot(probs[h], values_v[h]))
    kv_total = kv_src[block].astype(f32)
    for n in range(1, blocks):
        kv_total += kv_rx[n].astype(f32)
    kv_row = jnp.concatenate([kv_total[0:1], kv_total[1:2]], axis=1)
    kv_row = (jnp.broadcast_to(kv_row, (seqs, 2 * half_kv)) * inv_norm).astype(bf16).astype(f32)
    query_f32 = query_new.astype(f32)
    mine = lax.broadcasted_iota(jnp.int32, (seqs, 1), 0) == kv
    den_line = jnp.zeros((seqs, 128), f32)
    for h in range(heads):
        key_h = kv_row[:, h * key_size : (h + 1) * key_size]
        value_h = kv_row[:, width_q + h * value_size : width_q + (h + 1) * value_size]
        query_h = query_f32[:, h * key_size : (h + 1) * key_size]
        score = jnp.sum(query_h * key_h, axis=1, keepdims=True) * inv_root
        own = jnp.where(mine, own_weight[:, h : h + 1], 0.0)
        dens[h] += own * score
        nums[h] += (own * score.astype(bf16).astype(f32)) * value_h
        coarse = dens[h].astype(bf16).astype(f32)
        den_line = jnp.where(lane == h, coarse, den_line)
        den_line = jnp.where(lane == heads + h, dens[h] - coarse, den_line)
        span = pl.ds(h * value_size, value_size)
        part_src[:, span] = nums[h].astype(bf16)
        own_part[:, span] = nums[h]
    den_here = pl.ds(width_v, 128)
    part_src[:, den_here] = den_line.astype(bf16)
    own_part[:, den_here] = den_line
    for b in range(count_kv - 1, 0, -1):
        remote(part_src, part_rx.at[tp * count_kv + b], 3, 3, b * count_tp, lead)

    @pl.when(follows)
    def _():
        remote(part_src, part_rx.at[tp * count_kv], 3, 3, 0, lead)
        sent(part_rx.at[pl.ds(0, count_kv)], 3)
        sent(w_out, 7)

    @pl.when(leads)
    def _():
        arrived(part_rx.at[pl.ds(0, count_tp * count_kv - 1)], 3)
        for c in range(count_tp):
            def summed(span):
                held = [part_rx[c * count_kv + b, :, span].astype(f32) for b in range(1, count_kv)]
                held.append(own_part[:, span] if c == lead else part_rx[c * count_kv, :, span].astype(f32))
                return functools.reduce(jnp.add, held)

            tail = summed(den_here)
            for h in range(heads):
                den = tail[:, h : h + 1] + tail[:, heads + h : heads + h + 1]
                num = summed(pl.ds(h * value_size, value_size))
                span = pl.ds(c * width_v + h * value_size, value_size)
                heads_rx[dp, :, span] = (num / jnp.maximum(jnp.abs(den), 1.0)).astype(bf16)
        for a in range(1, count_dp):
            remote(heads_rx.at[dp], heads_rx.at[dp], 4, 4, a * count_kv * count_tp)
        loaded(wo_v.at[lead], 11)
        arrived(wo_v.at[pl.ds(0, count_tp - 1)], last + 1)
        arrived(heads_rx.at[pl.ds(0, count_dp - 1)], 4)
        lines = jnp.concatenate([heads_rx[a].astype(f32) for a in range(count_dp)], axis=0).astype(bf16)
        attended = jnp.concatenate([dot(lines, wo_v[c]) for c in range(count_tp)], axis=1)
        resid_rx[block] = (tok_v[...].astype(f32) + attended).astype(bf16)
        for r in near[::-1]:
            remote(resid_rx.at[block], resid_rx.at[block], 5, 5 + level_of[r], r)
        sent(part_rx.at[pl.ds(0, count_kv - 1)], 3)
        sent(heads_rx.at[pl.ds(0, count_dp - 1)], 4)

    loaded(gain_raw.at[1], 15)
    gains[1] = gain_raw[1].astype(f32)
    loaded(wgate_v, 12)
    loaded(wup_v, 13)
    gate_act = up_act = square = 0.0

    @pl.when(follows)
    def _():
        arrived(resid_rx.at[pl.ds(0, 1)], 5)

    for i in range(len(levels)):
        group = [r for r in range(0, count, count_tp) if level_of[r] == i]
        if i:
            arrived(resid_rx.at[pl.ds(0, len(group))], 5 + i)
        for r in group:
            at = place(r) // count_tp
            piece = resid_rx[at].astype(f32)
            square += jnp.sum(piece * piece, axis=1, keepdims=True)
            piece = (piece * gain_row(1, at, feat)).astype(bf16)
            span = pl.ds(pl.multiple_of(at * feat, feat), feat)
            gate_act += dot(piece, wgate_v[span, :])
            up_act += dot(piece, wup_v[span, :])
    inv_ffn = lax.rsqrt(square / model_width + epsilon)
    gate_act = gate_act * inv_ffn
    up_act = up_act * inv_ffn
    hidden = (gate_act / (1.0 + jnp.exp(-gate_act)) * up_act).astype(bf16)
    loaded(wdown_v, 14)
    def deliver(pair, results):
        for r, result in zip(pair, results):
            down_src[r] = result.astype(bf16)
        for r in pair:
            remote(down_src.at[r], down_rx.at[r], 6, last, r)

    order = near[::-1]
    pending = None
    for first in range(0, count - 1, 2):
        pair = order[first : first + 2]
        results = [dot(hidden, wdown_v[place(r)]) for r in pair]
        if pending:
            deliver(*pending)
        pending = (pair, results)
    total = dot(hidden, wdown_v[me])
    deliver(*pending)
    residual = resid_rx[block, :, pl.ds(pl.multiple_of(tp * out_block, out_block), out_block)]
    total += residual.astype(f32)
    sent(small_rx.at[pl.ds(1, blocks - 1)], 0)
    sent(q_rx.at[pl.ds(1, blocks - 1)], 1)
    sent(kv_rx.at[pl.ds(1, blocks - 1)], 2)

    @pl.when(leads)
    def _():
        for _ in range(count_tp):
            sent(resid_rx.at[pl.ds(0, blocks - 1)], 5)
        sent(resid_rx.at[pl.ds(0, count_tp - 1)], 5)

    arrived(down_rx.at[pl.ds(1, count - 1)], last)
    for r in near:
        total += down_rx[r].astype(f32)
    out_ref[...] = total.astype(bf16)
    sent(down_rx.at[pl.ds(1, count - 1)], 6)


def fused(
    tokens, lengths, cache_keys, cache_values, cache_igate, cache_fcum, gain_mix,
    w_query, w_key, w_value, w_gates, w_out, gain_ffn, w_gate, w_up, w_down,
):
    sizes = tuple(lax.axis_size(name) for name in ("dp", "kv", "tp"))
    count = sizes[0] * sizes[1] * sizes[2]
    blocks = sizes[0] * sizes[1]
    f32, bf16 = jnp.float32, jnp.bfloat16
    rows, feat = tokens.shape
    seqs, block_len, heads, key_size = cache_keys.shape
    value_size = cache_values.shape[3]
    out_block = w_out.shape[1]
    half_kv = heads * (key_size + value_size) // 2
    width_v = heads * value_size
    hbm = pl.BlockSpec(memory_space=pl.ANY)
    vmem = pl.BlockSpec(memory_space=pltpu.VMEM)
    dma = pltpu.SemaphoreType.DMA
    scratch = [
        pltpu.SMEM((seqs,), jnp.int32),
        pltpu.VMEM(tokens.shape, bf16),
        pltpu.VMEM((heads, seqs, block_len), f32),
        pltpu.VMEM((heads, seqs, block_len), f32),
        pltpu.VMEM((2, blocks * feat // 128, 128), bf16),
        pltpu.VMEM(w_query.shape, bf16),
        pltpu.VMEM(w_key.shape, bf16),
        pltpu.VMEM(w_value.shape, bf16),
        pltpu.VMEM((w_gates.shape[1], feat), bf16),
        pltpu.VMEM((sizes[2],) + w_out.shape, bf16),
        pltpu.VMEM(w_gate.shape, bf16),
        pltpu.VMEM(w_up.shape, bf16),
        pltpu.VMEM((count, w_down.shape[0], out_block), bf16),
        pltpu.VMEM((heads, seqs * block_len, key_size), bf16),
        pltpu.VMEM((heads, seqs * block_len, value_size), bf16),
        pltpu.VMEM((heads, key_size, seqs * block_len), bf16),
        pltpu.VMEM((sizes[0], seqs, heads * key_size), bf16),
        pltpu.VMEM((rows, 2, half_kv), bf16),
        pltpu.VMEM((sizes[0], seqs, 128), f32),
        pltpu.VMEM((blocks, seqs, heads * key_size), bf16),
        pltpu.VMEM((blocks, 2, half_kv), bf16),
        pltpu.VMEM((blocks, seqs, 128), f32),
        pltpu.VMEM((seqs, width_v + 128), f32),
        pltpu.VMEM((seqs, width_v + 128), bf16),
        pltpu.VMEM((sizes[2] * sizes[1], seqs, width_v + 128), bf16),
        pltpu.VMEM((sizes[0], seqs, sizes[2] * width_v), bf16),
        pltpu.VMEM((blocks, rows, feat), bf16),
        pltpu.VMEM((count, rows, out_block), bf16),
        pltpu.VMEM((count, rows, out_block), bf16),
        pltpu.VMEM((2, blocks * feat // 128, 128), f32),
        dma((16,)),
        dma((8,)),
        dma((5 + sizes[0] + sizes[1] - 1 + 2,)),
    ]
    operands = (
        lengths, tokens, cache_igate.swapaxes(0, 1), cache_fcum.swapaxes(0, 1),
        gain_mix.reshape(-1, 128), gain_ffn.reshape(-1, 128),
        cache_keys.swapaxes(1, 2), cache_values.swapaxes(1, 2),
        w_query, w_key, w_value, w_gates.T, w_out, w_gate, w_up, w_down,
    )
    return pl.pallas_call(
        functools.partial(fused_kernel, sizes),
        out_shape=pltpu.VMEM((rows, out_block), bf16),
        in_specs=[hbm] * len(operands),
        out_specs=vmem,
        scratch_shapes=scratch,
        compiler_params=pltpu.CompilerParams(
            collective_id=0, has_side_effects=True, vmem_limit_bytes=40 * 1024 * 1024
        ),
    )(*[pltpu.with_memory_space_constraint(x, pltpu.HBM) for x in operands])


def fits_kernel(tokens, cache_keys, w_out, w_gate):
    return (
        cache_keys.shape[0] == lax.axis_size("kv")
        and all(n in (2, 4) for n in map(lax.axis_size, ("dp", "kv", "tp")))
        and cache_keys.shape[2] <= 4
        and tokens.shape[1] % 128 == 0
        and w_out.shape[1] % 128 == 0
        and w_gate.shape[1] % 128 == 0
    )


def layer(*args):
    if fits_kernel(args[0], args[2], args[11], args[13]):
        return fused(*args)
    return per_device(*args)


def solution(mesh):
    in_specs = (
        P("grp", ("dp", "kv")),
        P(("grp", "dp")),
        P(("grp", "dp"), "kv", "tp", None),
        P(("grp", "dp"), "kv", "tp", None),
        P(("grp", "dp"), "tp", "kv"),
        P(("grp", "dp"), "tp", "kv"),
        P(),
        P(("dp", "kv"), "tp"),
        P(("dp", "kv"), "tp"),
        P(("dp", "kv"), "tp"),
        P(),
        P(None, ("dp", "kv", "tp")),
        P(),
        P(None, ("dp", "kv", "tp")),
        P(None, ("dp", "kv", "tp")),
        P(("dp", "kv", "tp"), None),
    )
    out_specs = P("grp", ("dp", "kv", "tp"))
    return jax.shard_map(
        layer, mesh=mesh, in_specs=in_specs, out_specs=out_specs, check_vma=False
    )
```

```python
import functools

import jax
import jax.numpy as jnp
from jax import lax
from jax.experimental import pallas as pl
from jax.experimental.pallas import tpu as pltpu
from jax.sharding import PartitionSpec as P

epsilon = 1e-06
very_low = -1e30


def combined_all(value, axis, join):
    pieces = jax.tree.map(lambda part: lax.all_gather(part, axis), value)
    head = jax.tree.map(lambda part: part[0], pieces)
    tail = jax.tree.map(lambda part: part[1:], pieces)
    total, _ = lax.scan(lambda total, piece: (join(total, piece), None), head, tail)
    return total


def merge_partial(first_part, second_part):
    max_first, den_first, num_first, anchor_first = first_part
    max_second, den_second, num_second, anchor_second = second_part
    highest = jnp.maximum(max_first, max_second)
    scale_first = jnp.exp(max_first - highest)
    scale_second = jnp.exp(max_second - highest)
    denominator = scale_first * den_first + scale_second * den_second
    numerator = scale_first[..., None] * num_first + scale_second[..., None] * num_second
    return (highest, denominator, numerator, jnp.maximum(anchor_first, anchor_second))


def per_device(
    tokens,
    lengths,
    cache_keys,
    cache_values,
    cache_igate,
    cache_fcum,
    gain_mix,
    w_query,
    w_key,
    w_value,
    w_gates,
    w_out,
    gain_ffn,
    w_gate,
    w_up,
    w_down,
):
    count_dp = lax.axis_size("dp")
    count_kv = lax.axis_size("kv")
    count_tp = lax.axis_size("tp")
    index_dp = lax.axis_index("dp")
    index_kv = lax.axis_index("kv")
    index_tp = lax.axis_index("tp")
    row_count, feat_block = tokens.shape
    seq_count, block_len, head_local, key_dimension = cache_keys.shape
    value_size = cache_values.shape[3]
    model_width = gain_mix.shape[0]
    heads_total = w_gates.shape[1] // 2
    out_block = w_out.shape[1]
    col_start = (index_dp * count_kv + index_kv) * feat_block
    token_f32 = tokens.astype(jnp.float32)
    gain_part = lax.dynamic_slice_in_dim(gain_mix, col_start, feat_block, 0).astype(jnp.float32)
    scaled = (token_f32 * gain_part[None, :]).astype(jnp.bfloat16)
    energy = jnp.sum(token_f32 * token_f32, axis=1)
    joined = jnp.concatenate(
        [
            jnp.dot(scaled, w_query, preferred_element_type=jnp.float32),
            jnp.dot(scaled, w_key, preferred_element_type=jnp.float32),
            jnp.dot(scaled, w_value, preferred_element_type=jnp.float32),
        ],
        axis=1,
    )
    gate_rows = lax.dynamic_slice_in_dim(w_gates, col_start, feat_block, 0).reshape(
        feat_block, 2, heads_total
    )
    gate_cols = lax.dynamic_slice_in_dim(gate_rows, index_tp * head_local, head_local, 2).reshape(
        feat_block, 2 * head_local
    )
    gate_part = jnp.dot(scaled, gate_cols, preferred_element_type=jnp.float32)
    joined_part, gate_rowsum, energy_part = (
        lax.psum_scatter(joined, "dp", scatter_dimension=0, tiled=True),
        lax.psum_scatter(gate_part, "dp", scatter_dimension=0, tiled=True),
        lax.psum_scatter(energy, "dp", scatter_dimension=0, tiled=True),
    )
    joined_own, gate_own, energy_own = lax.psum((joined_part, gate_rowsum, energy_part), "kv")
    inv_norm = lax.rsqrt(energy_own / model_width + epsilon)[:, None]
    width_qk = head_local * key_dimension
    query_new = (
        (joined_own[:, :width_qk] * inv_norm)
        .astype(jnp.bfloat16)
        .reshape(seq_count, head_local, key_dimension)
    )
    new_key = (
        (joined_own[:, width_qk : 2 * width_qk] * inv_norm)
        .astype(jnp.bfloat16)
        .reshape(seq_count, head_local, key_dimension)
    )
    new_value = (
        (joined_own[:, 2 * width_qk :] * inv_norm)
        .astype(jnp.bfloat16)
        .reshape(seq_count, head_local, value_size)
    )
    gates_now = gate_own * inv_norm
    in_gate = gates_now[:, :head_local]
    log_forget = jax.nn.log_sigmoid(gates_now[:, head_local:])
    inv_root = key_dimension ** (-0.5)
    scores = (
        jnp.einsum("shk,sphk->shp", query_new, cache_keys, preferred_element_type=jnp.float32)
        * inv_root
    )
    positions = index_kv * block_len + jnp.arange(block_len, dtype=jnp.int32)
    is_live = positions[None, None, :] < lengths[:, None, None]
    exponent = jnp.where(is_live, cache_igate - cache_fcum, very_low)
    block_max = jnp.max(exponent, axis=2)
    weight = jnp.where(is_live, jnp.exp(exponent - block_max[..., None]), 0.0)
    product = weight * scores
    block_den = jnp.sum(product, axis=2)
    block_num = jnp.einsum(
        "shp,sphv->shv",
        product.astype(jnp.bfloat16),
        cache_values,
        preferred_element_type=jnp.float32,
    )
    holding = positions[None, None, :] == (lengths - 1)[:, None, None]
    anchor = jnp.max(jnp.where(holding, cache_fcum, very_low), axis=2)
    cache_max, cache_den, cache_num, anchor_all = combined_all(
        (block_max, block_den, block_num, anchor), "kv", merge_partial
    )
    own_score = (
        jnp.sum(query_new.astype(jnp.float32) * new_key.astype(jnp.float32), axis=2) * inv_root
    )
    own_prob = lax.optimization_barrier(own_score.astype(jnp.bfloat16)).astype(jnp.float32)
    own_num = own_prob[..., None] * new_value.astype(jnp.float32)
    carried = anchor_all + log_forget
    highest = jnp.maximum(carried + cache_max, in_gate)
    weight_cache = jnp.exp(carried + cache_max - highest)
    weight_own = jnp.exp(in_gate - highest)
    denominator = weight_cache * cache_den + weight_own * own_score
    numerator = weight_cache[..., None] * cache_num + weight_own[..., None] * own_num
    heads_out = (numerator / jnp.maximum(jnp.abs(denominator), 1.0)[..., None]).astype(jnp.bfloat16)
    heads_out = heads_out.reshape(seq_count, head_local * value_size)
    gathered = lax.all_gather(heads_out[None], ("dp", "tp"), axis=0, tiled=True)
    gathered = gathered.reshape(count_dp, count_tp, seq_count, head_local * value_size)
    out_weight = w_out.reshape(count_tp, head_local * value_size, out_block)
    attended = jnp.einsum(
        "atsk,tkc->asc", gathered, out_weight, preferred_element_type=jnp.float32
    ).reshape(row_count, out_block)
    own_cols = lax.dynamic_slice_in_dim(token_f32, index_tp * out_block, out_block, 1)
    residual = (own_cols + attended).astype(jnp.bfloat16)
    full_rows = lax.all_gather(residual, ("dp", "kv", "tp"), axis=1, tiled=True)
    full_f32 = full_rows.astype(jnp.float32)
    inv_norm_ffn = lax.rsqrt(jnp.mean(full_f32 * full_f32, axis=1, keepdims=True) + epsilon)
    normed = (full_f32 * inv_norm_ffn * gain_ffn.astype(jnp.float32)[None, :]).astype(jnp.bfloat16)
    gate_act = jnp.dot(normed, w_gate, preferred_element_type=jnp.float32)
    up_act = jnp.dot(normed, w_up, preferred_element_type=jnp.float32)
    hidden = (jax.nn.silu(gate_act) * up_act).astype(jnp.bfloat16)
    summed = lax.psum_scatter(
        lax.dot_general(
            w_down, hidden, (((0,), (1,)), ((), ())), preferred_element_type=jnp.float32
        ),
        ("dp", "kv", "tp"),
        scatter_dimension=0,
        tiled=True,
    )
    return (residual.astype(jnp.float32) + summed.T).astype(jnp.bfloat16)


def fused_kernel(
    sizes, lengths, tokens, cache_igate, cache_fcum, gain_mix, gain_ffn,
    cache_keys, cache_values, w_query, w_key, w_value, w_gates, w_out, w_gate, w_up, w_down,
    out_ref,
    len_s, tok_v, igate_v, fcum_v, gain_raw,
    wq_v, wk_v, wv_v, wg_v, wo_v, wgate_v, wup_v, wdown_v,
    keys_v, values_v,
    keys_t, q_src, kv_src, small_src, q_rx, kv_rx, small_rx,
    own_part, part_src, part_rx, heads_rx, resid_rx, down_src, down_rx, gains,
    load_sem, send_sem, recv_sem,
):
    count_dp, count_kv, count_tp = sizes
    count = count_dp * count_kv * count_tp
    blocks = count_dp * count_kv
    dp, kv, tp = lax.axis_index("dp"), lax.axis_index("kv"), lax.axis_index("tp")
    f32, bf16 = jnp.float32, jnp.bfloat16
    seqs, heads, block_len, key_size = cache_keys.shape
    value_size = cache_values.shape[3]
    rows, feat = tokens.shape
    width_q = heads * key_size
    width_v = heads * value_size
    half_kv = (width_q + width_v) // 2
    out_block = out_ref.shape[1]
    model_width = feat * blocks
    heads_total = heads * count_tp
    block = dp * count_kv + kv
    me = block * count_tp + tp
    lead = count_tp - 1
    leads, follows = tp == lead, tp != lead

    inner = (kv ^ (kv >> 1)) & 1
    by_reach = {i: i for i in range(count_kv)}
    if count_kv == 4:
        by_reach = {i: i + inner * (b - i) for i, b in enumerate((0, 3, 1, 2))}

    def step(r):
        return r // (count_kv * count_tp), by_reach[(r // count_tp) % count_kv], r % count_tp

    def target(r):
        a, b, c = step(r)
        return dp ^ a, kv ^ b, tp ^ c

    def place(r):
        t = target(r)
        return (t[0] * count_kv + t[1]) * count_tp + t[2]

    def slot(r):
        a, b, c = step(r)
        return (a * count_kv + b) * count_tp + c

    def device(r):
        t = target(r)
        return {"dp": t[0], "kv": t[1], "tp": t[2]}

    def level(r):
        return r // (count_kv * count_tp) + (r // count_tp) % count_kv

    def level_there(r):
        here = (r // count_tp) % count_kv
        if count_kv != 4:
            return level(r)
        outer, inside = ((0, 2, 3, 3), (0, 1, 1, 2))
        return r // (count_kv * count_tp) + outer[here] + inner * (inside[here] - outer[here])

    near = sorted(range(1, count), key=lambda r: (level(r), r % count_tp))
    levels = count_dp + count_kv - 1
    last = 5 + levels
    peers = sorted(range(count_tp, count, count_tp), key=level)[::-1]

    def gain_row(which, at, width):
        lines = width // 128
        first = at * lines
        return jnp.concatenate(
            [gains[which, pl.ds(first + i, 1), :] for i in range(lines)], axis=1
        )

    def load(hbm, vmem, index, pieces=1):
        step = hbm.shape[0] // pieces
        for i in range(pieces):
            pltpu.make_async_copy(
                hbm.at[pl.ds(i * step, step)], vmem.at[pl.ds(i * step, step)], load_sem.at[index]
            ).start()

    def loaded(vmem, index):
        pltpu.make_async_copy(vmem, vmem, load_sem.at[index]).wait()

    def remote(src, dst, send, recv, r, core=None):
        where = device(r)
        if core is not None:
            where["tp"] = core
        pltpu.make_async_remote_copy(
            src_ref=src, dst_ref=dst, send_sem=send_sem.at[send], recv_sem=recv_sem.at[recv],
            device_id=where, device_id_type=pl.DeviceIdType.MESH,
        ).start()

    def arrived(like, recv):
        pltpu.make_async_copy(like, like, recv_sem.at[recv]).wait()

    def sent(like, send):
        pltpu.make_async_copy(like, like, send_sem.at[send]).wait()

    barrier = pltpu.get_barrier_semaphore()
    for r in near[::-1]:
        pl.semaphore_signal(
            barrier, inc=1, device_id=device(r), device_id_type=pl.DeviceIdType.MESH
        )
    load(tokens, tok_v, 0)
    load(gain_mix, gain_raw.at[0], 0)
    gate_start = pl.multiple_of(block * feat, feat)
    pltpu.make_async_copy(w_gates.at[:, pl.ds(gate_start, feat)], wg_v, load_sem.at[0]).start()
    load(w_query, wq_v, 2, 4)
    load(lengths, len_s, 1)
    load(cache_igate, igate_v, 1)
    load(cache_fcum, fcum_v, 1)
    load(w_key, wk_v, 3, 2)
    load(w_value, wv_v, 3, 4)

    dot = functools.partial(jnp.dot, preferred_element_type=f32)
    loaded(tok_v, 0)
    loaded(gain_raw.at[0], 0)
    loaded(wg_v, 0)
    gains[0] = gain_raw[0].astype(f32)
    token = tok_v[...].astype(f32)
    scaled = (token * gain_row(0, block, feat)).astype(bf16)
    energy = jnp.sum(token * token, axis=1, keepdims=True)
    gate_part = lax.dot_general(
        scaled, wg_v[...], (((1,), (1,)), ((), ())), preferred_element_type=f32
    )
    gate_part = jnp.concatenate(
        [gate_part, jnp.zeros((rows, 128 - 2 * heads_total), f32)], axis=1
    )
    shifted = gate_part
    for c in range(1, count_tp):
        shifted = jnp.where(tp == c, pltpu.roll(gate_part, 128 - c * heads, 1), shifted)
    lane_all = lax.broadcasted_iota(jnp.int32, (rows, 128), 1)
    at_energy, at_max, at_anchor = 16, 32, 64
    shifted = jnp.where(lane_all == at_energy, energy, shifted)

    loaded(len_s, 1)
    loaded(igate_v, 1)
    loaded(fcum_v, 1)
    lane = lax.broadcasted_iota(jnp.int32, (seqs, 128), 1)
    row = lax.broadcasted_iota(jnp.int32, (seqs, block_len), 0)
    row_v = lax.broadcasted_iota(jnp.int32, (seqs, value_size), 0)
    length = jnp.zeros((seqs, block_len), jnp.int32)
    for s in range(seqs):
        length = jnp.where(row == s, len_s[s], length)
    position = kv * block_len + lax.broadcasted_iota(jnp.int32, (seqs, block_len), 1)
    live = position < length
    holding = position == length - 1
    exponents = []
    stats = jnp.full((seqs, 128), very_low, f32)
    for h in range(heads):
        fcum = fcum_v[h]
        exponent = jnp.where(live, igate_v[h] - fcum, very_low)
        exponents.append(exponent)
        top = jnp.max(exponent, axis=1, keepdims=True)
        anchor = jnp.max(jnp.where(holding, fcum, very_low), axis=1, keepdims=True)
        stats = jnp.where(lane == at_max + h, top, stats)
        stats = jnp.where(lane == at_anchor + h, anchor, stats)
    for a in range(count_dp):
        part = shifted[a * seqs : (a + 1) * seqs]
        small_src[a] = jnp.where(lane < at_max, part, stats)

    loaded(wq_v, 2)
    query = dot(scaled, wq_v[...])
    for a in range(count_dp):
        q_src[a] = query[a * seqs : (a + 1) * seqs].astype(bf16)
    def keys_and_values():
        loaded(wk_v, 3)
        loaded(wv_v, 3)
        joined = jnp.concatenate([dot(scaled, wk_v[...]), dot(scaled, wv_v[...])], axis=1)
        for i in range(rows):
            line = joined[i : i + 1]
            kv_src[i] = jnp.concatenate([line[:, :half_kv], line[:, half_kv:]], axis=0).astype(bf16)

    pl.when(kv == 0)(keys_and_values)
    pl.semaphore_wait(barrier, count - 1)

    def send_query(r):
        n, to = slot(r) // count_tp, target(r)[0]
        remote(small_src.at[to], small_rx.at[n], 0, 0, r)
        remote(q_src.at[to], q_rx.at[n], 1, 1, r)

    def send_values(r):
        t = target(r)
        remote(kv_src.at[t[0] * count_kv + t[1]], kv_rx.at[slot(r) // count_tp], 2, 2, r)

    @pl.when(kv == 0)
    def _():
        for r in peers:
            send_query(r)
            send_values(r)

    @pl.when(kv != 0)
    def _():
        for r in peers:
            send_query(r)

    for s in range(seqs):
        span = pl.ds(s * block_len, block_len)
        pltpu.make_async_copy(cache_keys.at[s], keys_v.at[:, span, :], load_sem.at[4]).start()
    for s in range(seqs):
        span = pl.ds(s * block_len, block_len)
        pltpu.make_async_copy(cache_values.at[s], values_v.at[:, span, :], load_sem.at[5]).start()
    @pl.when(kv != 0)
    def _():
        keys_and_values()
        for r in peers:
            send_values(r)

    @pl.when(follows)
    def _():
        remote(w_out, wo_v.at[tp], 7, last + 1, 0, lead)

    @pl.when(leads)
    def _():
        load(w_out, wo_v.at[lead], 6, 4)

    load(gain_ffn, gain_raw.at[1], 7)
    load(w_gate, wgate_v, 8, 8)
    load(w_up, wup_v, 8, 8)
    for j in range(count):
        pltpu.make_async_copy(
            w_down.at[:, pl.ds(j * out_block, out_block)], wdown_v.at[j], load_sem.at[9]
        ).start()

    loaded(keys_v, 4)
    for h in range(heads):
        keys_t[h] = keys_v[h].T

    arrived(small_rx.at[pl.ds(1, blocks - 1)], 0)
    arrived(q_rx.at[pl.ds(1, blocks - 1)], 1)
    small = small_src[dp]
    extreme = small
    for n in range(1, blocks):
        small += small_rx[n]
        if n < count_kv:
            extreme = jnp.maximum(extreme, small_rx[n])
    inv_norm = lax.rsqrt(small[:, at_energy : at_energy + 1] / model_width + epsilon)
    q_total = q_src[dp].astype(f32)
    for n in range(1, blocks):
        q_total += q_rx[n].astype(f32)
    query_new = (q_total * inv_norm).astype(bf16)
    founds = [
        dot(query_new[:, h * key_size : (h + 1) * key_size], keys_t[h]) for h in range(heads)
    ]
    gates_now = small * inv_norm
    log_forget = jnp.minimum(gates_now, 0.0) - jnp.log1p(jnp.exp(-jnp.abs(gates_now)))
    forget_here = pltpu.roll(log_forget, 128 - heads_total, 1)
    top_here = pltpu.roll(extreme, 128 - at_max, 1)
    carried = pltpu.roll(extreme, 128 - at_anchor, 1) + forget_here
    highest = jnp.maximum(carried + top_here, gates_now)
    offset = carried - highest
    own_weight = jnp.exp(gates_now - highest)
    weights = []
    for h in range(heads):
        power = jnp.where(live, exponents[h] + offset[:, h : h + 1], very_low)
        weights.append(jnp.where(live, jnp.exp(power), 0.0))

    inv_root = key_size ** (-0.5)
    probs, dens, nums = [], [], []
    for h in range(heads):
        found = founds[h]
        score = found[:, 0:block_len]
        for s in range(1, seqs):
            score = jnp.where(row == s, found[:, s * block_len : (s + 1) * block_len], score)
        product = weights[h] * (score * inv_root)
        dens.append(jnp.sum(product, axis=1, keepdims=True))
        probs.append(
            jnp.concatenate([jnp.where(row == s, product, 0.0) for s in range(seqs)], axis=1).astype(bf16)
        )
    loaded(values_v, 5)
    arrived(kv_rx.at[pl.ds(1, blocks - 1)], 2)
    for h in range(heads):
        nums.append(dot(probs[h], values_v[h]))
    kv_total = kv_src[block].astype(f32)
    for n in range(1, blocks):
        kv_total += kv_rx[n].astype(f32)
    kv_row = jnp.concatenate([kv_total[0:1], kv_total[1:2]], axis=1)
    kv_row = (jnp.broadcast_to(kv_row, (seqs, 2 * half_kv)) * inv_norm).astype(bf16).astype(f32)
    query_f32 = query_new.astype(f32)
    mine = lax.broadcasted_iota(jnp.int32, (seqs, 1), 0) == kv
    den_line = jnp.zeros((seqs, 128), f32)
    for h in range(heads):
        key_h = kv_row[:, h * key_size : (h + 1) * key_size]
        value_h = kv_row[:, width_q + h * value_size : width_q + (h + 1) * value_size]
        query_h = query_f32[:, h * key_size : (h + 1) * key_size]
        score = jnp.sum(query_h * key_h, axis=1, keepdims=True) * inv_root
        own = jnp.where(mine, own_weight[:, h : h + 1], 0.0)
        dens[h] += own * score
        nums[h] += (own * score.astype(bf16).astype(f32)) * value_h
        coarse = dens[h].astype(bf16).astype(f32)
        den_line = jnp.where(lane == h, coarse, den_line)
        den_line = jnp.where(lane == heads + h, dens[h] - coarse, den_line)
        span = pl.ds(h * value_size, value_size)
        part_src[:, span] = nums[h].astype(bf16)
        own_part[:, span] = nums[h]
    den_here = pl.ds(width_v, 128)
    part_src[:, den_here] = den_line.astype(bf16)
    own_part[:, den_here] = den_line
    for b in range(count_kv - 1, 0, -1):
        remote(part_src, part_rx.at[tp * count_kv + by_reach[b]], 3, 3, b * count_tp, lead)

    @pl.when(follows)
    def _():
        remote(part_src, part_rx.at[tp * count_kv], 3, 3, 0, lead)
        sent(part_rx.at[pl.ds(0, count_kv)], 3)
        sent(w_out, 7)

    @pl.when(leads)
    def _():
        arrived(part_rx.at[pl.ds(0, count_tp * count_kv - 1)], 3)
        for c in range(count_tp):
            def summed(span):
                held = [part_rx[c * count_kv + b, :, span].astype(f32) for b in range(1, count_kv)]
                held.append(own_part[:, span] if c == lead else part_rx[c * count_kv, :, span].astype(f32))
                return functools.reduce(jnp.add, held)

            tail = summed(den_here)
            for h in range(heads):
                den = tail[:, h : h + 1] + tail[:, heads + h : heads + h + 1]
                num = summed(pl.ds(h * value_size, value_size))
                span = pl.ds(c * width_v + h * value_size, value_size)
                heads_rx[dp, :, span] = (num / jnp.maximum(jnp.abs(den), 1.0)).astype(bf16)
        for a in range(1, count_dp):
            remote(heads_rx.at[dp], heads_rx.at[dp], 4, 4, a * count_kv * count_tp)
        loaded(wo_v.at[lead], 6)
        arrived(wo_v.at[pl.ds(0, count_tp - 1)], last + 1)
        arrived(heads_rx.at[pl.ds(0, count_dp - 1)], 4)
        lines = jnp.concatenate([heads_rx[a].astype(f32) for a in range(count_dp)], axis=0).astype(bf16)
        attended = jnp.concatenate([dot(lines, wo_v[c]) for c in range(count_tp)], axis=1)
        resid_rx[block] = (tok_v[...].astype(f32) + attended).astype(bf16)
        for r in near[::-1]:
            remote(resid_rx.at[block], resid_rx.at[block], 5, 5 + level_there(r), r)
        sent(part_rx.at[pl.ds(0, count_kv - 1)], 3)
        sent(heads_rx.at[pl.ds(0, count_dp - 1)], 4)

    loaded(gain_raw.at[1], 7)
    gains[1] = gain_raw[1].astype(f32)
    loaded(wgate_v, 8)
    loaded(wup_v, 8)
    gate_act = up_act = square = 0.0

    @pl.when(follows)
    def _():
        arrived(resid_rx.at[pl.ds(0, 1)], 5)

    for i in range(levels):
        group = [r for r in range(0, count, count_tp) if level(r) == i]
        if i:
            arrived(resid_rx.at[pl.ds(0, len(group))], 5 + i)
        for r in group:
            at = place(r) // count_tp
            piece = resid_rx[at].astype(f32)
            square += jnp.sum(piece * piece, axis=1, keepdims=True)
            piece = (piece * gain_row(1, at, feat)).astype(bf16)
            span = pl.ds(pl.multiple_of(at * feat, feat), feat)
            gate_act += dot(piece, wgate_v[span, :])
            up_act += dot(piece, wup_v[span, :])
    inv_ffn = lax.rsqrt(square / model_width + epsilon)
    gate_act = gate_act * inv_ffn
    up_act = up_act * inv_ffn
    hidden = (gate_act / (1.0 + jnp.exp(-gate_act)) * up_act).astype(bf16)
    loaded(wdown_v, 9)
    def deliver(pair, results):
        for r, result in zip(pair, results):
            down_src[r] = result.astype(bf16)
        for r in pair:
            remote(down_src.at[r], down_rx.at[slot(r)], 6, last, r)

    order = near[::-1]
    pending = None
    for first in range(0, count - 1, 2):
        pair = order[first : first + 2]
        results = [dot(hidden, wdown_v[place(r)]) for r in pair]
        if pending:
            deliver(*pending)
        pending = (pair, results)
    total = dot(hidden, wdown_v[me])
    deliver(*pending)
    residual = resid_rx[block, :, pl.ds(pl.multiple_of(tp * out_block, out_block), out_block)]
    total += residual.astype(f32)
    sent(small_rx.at[pl.ds(1, blocks - 1)], 0)
    sent(q_rx.at[pl.ds(1, blocks - 1)], 1)
    sent(kv_rx.at[pl.ds(1, blocks - 1)], 2)

    @pl.when(leads)
    def _():
        for _ in range(count_tp):
            sent(resid_rx.at[pl.ds(0, blocks - 1)], 5)
        sent(resid_rx.at[pl.ds(0, count_tp - 1)], 5)

    arrived(down_rx.at[pl.ds(1, count - 1)], last)
    for r in near:
        total += down_rx[r].astype(f32)
    out_ref[...] = total.astype(bf16)
    sent(down_rx.at[pl.ds(1, count - 1)], 6)


def fused(
    tokens, lengths, cache_keys, cache_values, cache_igate, cache_fcum, gain_mix,
    w_query, w_key, w_value, w_gates, w_out, gain_ffn, w_gate, w_up, w_down,
):
    sizes = tuple(lax.axis_size(name) for name in ("dp", "kv", "tp"))
    count = sizes[0] * sizes[1] * sizes[2]
    blocks = sizes[0] * sizes[1]
    f32, bf16 = jnp.float32, jnp.bfloat16
    rows, feat = tokens.shape
    seqs, block_len, heads, key_size = cache_keys.shape
    value_size = cache_values.shape[3]
    out_block = w_out.shape[1]
    half_kv = heads * (key_size + value_size) // 2
    width_v = heads * value_size
    hbm = pl.BlockSpec(memory_space=pl.ANY)
    vmem = pl.BlockSpec(memory_space=pltpu.VMEM)
    dma = pltpu.SemaphoreType.DMA
    scratch = [
        pltpu.SMEM((seqs,), jnp.int32),
        pltpu.VMEM(tokens.shape, bf16),
        pltpu.VMEM((heads, seqs, block_len), f32),
        pltpu.VMEM((heads, seqs, block_len), f32),
        pltpu.VMEM((2, blocks * feat // 128, 128), bf16),
        pltpu.VMEM(w_query.shape, bf16),
        pltpu.VMEM(w_key.shape, bf16),
        pltpu.VMEM(w_value.shape, bf16),
        pltpu.VMEM((w_gates.shape[1], feat), bf16),
        pltpu.VMEM((sizes[2],) + w_out.shape, bf16),
        pltpu.VMEM(w_gate.shape, bf16),
        pltpu.VMEM(w_up.shape, bf16),
        pltpu.VMEM((count, w_down.shape[0], out_block), bf16),
        pltpu.VMEM((heads, seqs * block_len, key_size), bf16),
        pltpu.VMEM((heads, seqs * block_len, value_size), bf16),
        pltpu.VMEM((heads, key_size, seqs * block_len), bf16),
        pltpu.VMEM((sizes[0], seqs, heads * key_size), bf16),
        pltpu.VMEM((rows, 2, half_kv), bf16),
        pltpu.VMEM((sizes[0], seqs, 128), f32),
        pltpu.VMEM((blocks, seqs, heads * key_size), bf16),
        pltpu.VMEM((blocks, 2, half_kv), bf16),
        pltpu.VMEM((blocks, seqs, 128), f32),
        pltpu.VMEM((seqs, width_v + 128), f32),
        pltpu.VMEM((seqs, width_v + 128), bf16),
        pltpu.VMEM((sizes[2] * sizes[1], seqs, width_v + 128), bf16),
        pltpu.VMEM((sizes[0], seqs, sizes[2] * width_v), bf16),
        pltpu.VMEM((blocks, rows, feat), bf16),
        pltpu.VMEM((count, rows, out_block), bf16),
        pltpu.VMEM((count, rows, out_block), bf16),
        pltpu.VMEM((2, blocks * feat // 128, 128), f32),
        dma((10,)),
        dma((8,)),
        dma((5 + sizes[0] + sizes[1] - 1 + 2,)),
    ]
    operands = (
        lengths, tokens, cache_igate.swapaxes(0, 1), cache_fcum.swapaxes(0, 1),
        gain_mix.reshape(-1, 128), gain_ffn.reshape(-1, 128),
        cache_keys.swapaxes(1, 2), cache_values.swapaxes(1, 2),
        w_query, w_key, w_value, w_gates.T, w_out, w_gate, w_up, w_down,
    )
    return pl.pallas_call(
        functools.partial(fused_kernel, sizes),
        out_shape=pltpu.VMEM((rows, out_block), bf16),
        in_specs=[hbm] * len(operands),
        out_specs=vmem,
        scratch_shapes=scratch,
        compiler_params=pltpu.CompilerParams(
            collective_id=0, has_side_effects=True, vmem_limit_bytes=40 * 1024 * 1024
        ),
    )(*[pltpu.with_memory_space_constraint(x, pltpu.HBM) for x in operands])


def fits_kernel(tokens, cache_keys, w_out, w_gate):
    return (
        cache_keys.shape[0] == lax.axis_size("kv")
        and all(n in (2, 4) for n in map(lax.axis_size, ("dp", "kv", "tp")))
        and cache_keys.shape[2] <= 4
        and tokens.shape[1] % 128 == 0
        and w_out.shape[1] % 128 == 0
        and w_gate.shape[1] % 128 == 0
    )


def layer(*args):
    if fits_kernel(args[0], args[2], args[11], args[13]):
        return fused(*args)
    return per_device(*args)


def solution(mesh):
    in_specs = (
        P("grp", ("dp", "kv")),
        P(("grp", "dp")),
        P(("grp", "dp"), "kv", "tp", None),
        P(("grp", "dp"), "kv", "tp", None),
        P(("grp", "dp"), "tp", "kv"),
        P(("grp", "dp"), "tp", "kv"),
        P(),
        P(("dp", "kv"), "tp"),
        P(("dp", "kv"), "tp"),
        P(("dp", "kv"), "tp"),
        P(),
        P(None, ("dp", "kv", "tp")),
        P(),
        P(None, ("dp", "kv", "tp")),
        P(None, ("dp", "kv", "tp")),
        P(("dp", "kv", "tp"), None),
    )
    out_specs = P("grp", ("dp", "kv", "tp"))
    return jax.shard_map(
        layer, mesh=mesh, in_specs=in_specs, out_specs=out_specs, check_vma=False
    )
```

```python
import functools

import jax
import jax.numpy as jnp
from jax import lax
from jax.experimental import pallas as pl
from jax.experimental.pallas import tpu as pltpu
from jax.sharding import PartitionSpec as P

epsilon = 1e-06
very_low = -1e30


def combined_all(value, axis, join):
    pieces = jax.tree.map(lambda part: lax.all_gather(part, axis), value)
    head = jax.tree.map(lambda part: part[0], pieces)
    tail = jax.tree.map(lambda part: part[1:], pieces)
    total, _ = lax.scan(lambda total, piece: (join(total, piece), None), head, tail)
    return total


def merge_partial(first_part, second_part):
    max_first, den_first, num_first, anchor_first = first_part
    max_second, den_second, num_second, anchor_second = second_part
    highest = jnp.maximum(max_first, max_second)
    scale_first = jnp.exp(max_first - highest)
    scale_second = jnp.exp(max_second - highest)
    denominator = scale_first * den_first + scale_second * den_second
    numerator = scale_first[..., None] * num_first + scale_second[..., None] * num_second
    return (highest, denominator, numerator, jnp.maximum(anchor_first, anchor_second))


def per_device(
    tokens,
    lengths,
    cache_keys,
    cache_values,
    cache_igate,
    cache_fcum,
    gain_mix,
    w_query,
    w_key,
    w_value,
    w_gates,
    w_out,
    gain_ffn,
    w_gate,
    w_up,
    w_down,
):
    count_dp = lax.axis_size("dp")
    count_kv = lax.axis_size("kv")
    count_tp = lax.axis_size("tp")
    index_dp = lax.axis_index("dp")
    index_kv = lax.axis_index("kv")
    index_tp = lax.axis_index("tp")
    row_count, feat_block = tokens.shape
    seq_count, block_len, head_local, key_dimension = cache_keys.shape
    value_size = cache_values.shape[3]
    model_width = gain_mix.shape[0]
    heads_total = w_gates.shape[1] // 2
    out_block = w_out.shape[1]
    col_start = (index_dp * count_kv + index_kv) * feat_block
    token_f32 = tokens.astype(jnp.float32)
    gain_part = lax.dynamic_slice_in_dim(gain_mix, col_start, feat_block, 0).astype(jnp.float32)
    scaled = (token_f32 * gain_part[None, :]).astype(jnp.bfloat16)
    energy = jnp.sum(token_f32 * token_f32, axis=1)
    joined = jnp.concatenate(
        [
            jnp.dot(scaled, w_query, preferred_element_type=jnp.float32),
            jnp.dot(scaled, w_key, preferred_element_type=jnp.float32),
            jnp.dot(scaled, w_value, preferred_element_type=jnp.float32),
        ],
        axis=1,
    )
    gate_rows = lax.dynamic_slice_in_dim(w_gates, col_start, feat_block, 0).reshape(
        feat_block, 2, heads_total
    )
    gate_cols = lax.dynamic_slice_in_dim(gate_rows, index_tp * head_local, head_local, 2).reshape(
        feat_block, 2 * head_local
    )
    gate_part = jnp.dot(scaled, gate_cols, preferred_element_type=jnp.float32)
    joined_part, gate_rowsum, energy_part = (
        lax.psum_scatter(joined, "dp", scatter_dimension=0, tiled=True),
        lax.psum_scatter(gate_part, "dp", scatter_dimension=0, tiled=True),
        lax.psum_scatter(energy, "dp", scatter_dimension=0, tiled=True),
    )
    joined_own, gate_own, energy_own = lax.psum((joined_part, gate_rowsum, energy_part), "kv")
    inv_norm = lax.rsqrt(energy_own / model_width + epsilon)[:, None]
    width_qk = head_local * key_dimension
    query_new = (
        (joined_own[:, :width_qk] * inv_norm)
        .astype(jnp.bfloat16)
        .reshape(seq_count, head_local, key_dimension)
    )
    new_key = (
        (joined_own[:, width_qk : 2 * width_qk] * inv_norm)
        .astype(jnp.bfloat16)
        .reshape(seq_count, head_local, key_dimension)
    )
    new_value = (
        (joined_own[:, 2 * width_qk :] * inv_norm)
        .astype(jnp.bfloat16)
        .reshape(seq_count, head_local, value_size)
    )
    gates_now = gate_own * inv_norm
    in_gate = gates_now[:, :head_local]
    log_forget = jax.nn.log_sigmoid(gates_now[:, head_local:])
    inv_root = key_dimension ** (-0.5)
    scores = (
        jnp.einsum("shk,sphk->shp", query_new, cache_keys, preferred_element_type=jnp.float32)
        * inv_root
    )
    positions = index_kv * block_len + jnp.arange(block_len, dtype=jnp.int32)
    is_live = positions[None, None, :] < lengths[:, None, None]
    exponent = jnp.where(is_live, cache_igate - cache_fcum, very_low)
    block_max = jnp.max(exponent, axis=2)
    weight = jnp.where(is_live, jnp.exp(exponent - block_max[..., None]), 0.0)
    product = weight * scores
    block_den = jnp.sum(product, axis=2)
    block_num = jnp.einsum(
        "shp,sphv->shv",
        product.astype(jnp.bfloat16),
        cache_values,
        preferred_element_type=jnp.float32,
    )
    holding = positions[None, None, :] == (lengths - 1)[:, None, None]
    anchor = jnp.max(jnp.where(holding, cache_fcum, very_low), axis=2)
    cache_max, cache_den, cache_num, anchor_all = combined_all(
        (block_max, block_den, block_num, anchor), "kv", merge_partial
    )
    own_score = (
        jnp.sum(query_new.astype(jnp.float32) * new_key.astype(jnp.float32), axis=2) * inv_root
    )
    own_prob = lax.optimization_barrier(own_score.astype(jnp.bfloat16)).astype(jnp.float32)
    own_num = own_prob[..., None] * new_value.astype(jnp.float32)
    carried = anchor_all + log_forget
    highest = jnp.maximum(carried + cache_max, in_gate)
    weight_cache = jnp.exp(carried + cache_max - highest)
    weight_own = jnp.exp(in_gate - highest)
    denominator = weight_cache * cache_den + weight_own * own_score
    numerator = weight_cache[..., None] * cache_num + weight_own[..., None] * own_num
    heads_out = (numerator / jnp.maximum(jnp.abs(denominator), 1.0)[..., None]).astype(jnp.bfloat16)
    heads_out = heads_out.reshape(seq_count, head_local * value_size)
    gathered = lax.all_gather(heads_out[None], ("dp", "tp"), axis=0, tiled=True)
    gathered = gathered.reshape(count_dp, count_tp, seq_count, head_local * value_size)
    out_weight = w_out.reshape(count_tp, head_local * value_size, out_block)
    attended = jnp.einsum(
        "atsk,tkc->asc", gathered, out_weight, preferred_element_type=jnp.float32
    ).reshape(row_count, out_block)
    own_cols = lax.dynamic_slice_in_dim(token_f32, index_tp * out_block, out_block, 1)
    residual = (own_cols + attended).astype(jnp.bfloat16)
    full_rows = lax.all_gather(residual, ("dp", "kv", "tp"), axis=1, tiled=True)
    full_f32 = full_rows.astype(jnp.float32)
    inv_norm_ffn = lax.rsqrt(jnp.mean(full_f32 * full_f32, axis=1, keepdims=True) + epsilon)
    normed = (full_f32 * inv_norm_ffn * gain_ffn.astype(jnp.float32)[None, :]).astype(jnp.bfloat16)
    gate_act = jnp.dot(normed, w_gate, preferred_element_type=jnp.float32)
    up_act = jnp.dot(normed, w_up, preferred_element_type=jnp.float32)
    hidden = (jax.nn.silu(gate_act) * up_act).astype(jnp.bfloat16)
    summed = lax.psum_scatter(
        lax.dot_general(
            w_down, hidden, (((0,), (1,)), ((), ())), preferred_element_type=jnp.float32
        ),
        ("dp", "kv", "tp"),
        scatter_dimension=0,
        tiled=True,
    )
    return (residual.astype(jnp.float32) + summed.T).astype(jnp.bfloat16)


def fused_kernel(
    sizes, lengths, tokens, cache_igate, cache_fcum, gain_mix, gain_ffn,
    cache_keys, cache_values, w_query, w_key, w_value, w_gates, w_out, w_gate, w_up, w_down,
    out_ref,
    len_s, tok_v, igate_v, fcum_v, gain_raw,
    wq_v, wk_v, wv_v, wg_v, wo_v, wgate_v, wup_v, wdown_v,
    keys_v, values_v,
    keys_t, q_src, kv_src, small_src, q_rx, kv_rx, small_rx, q_via, kv_via, small_via,
    acc_v, own_part, part_src, part_rx, heads_rx, resid_rx, down_src, down_rx, gains,
    load_sem, send_sem, recv_sem,
):
    count_dp, count_kv, count_tp = sizes
    count = count_dp * count_kv * count_tp
    blocks = count_dp * count_kv
    dp, kv, tp = lax.axis_index("dp"), lax.axis_index("kv"), lax.axis_index("tp")
    f32, bf16 = jnp.float32, jnp.bfloat16
    seqs, heads, block_len, key_size = cache_keys.shape
    value_size = cache_values.shape[3]
    rows, feat = tokens.shape
    width_q = heads * key_size
    width_v = heads * value_size
    half_kv = (width_q + width_v) // 2
    out_block = out_ref.shape[1]
    model_width = feat * blocks
    heads_total = heads * count_tp
    block = dp * count_kv + kv
    me = block * count_tp + tp
    lead = count_tp - 1
    leads, follows = tp == lead, tp != lead

    inner = (kv ^ (kv >> 1)) & 1
    by_reach = {i: i for i in range(count_kv)}
    if count_kv == 4:
        by_reach = {i: i + inner * (b - i) for i, b in enumerate((0, 3, 1, 2))}

    def step(r):
        return r // (count_kv * count_tp), by_reach[(r // count_tp) % count_kv], r % count_tp

    def target(r):
        a, b, c = step(r)
        return dp ^ a, kv ^ b, tp ^ c

    def place(r):
        t = target(r)
        return (t[0] * count_kv + t[1]) * count_tp + t[2]

    def slot(r):
        a, b, c = step(r)
        return (a * count_kv + b) * count_tp + c

    def device(r):
        t = target(r)
        return {"dp": t[0], "kv": t[1], "tp": t[2]}

    def level(r):
        return r // (count_kv * count_tp) + (r // count_tp) % count_kv

    def level_there(r):
        here = (r // count_tp) % count_kv
        if count_kv != 4:
            return level(r)
        outer, inside = ((0, 2, 3, 3), (0, 1, 1, 2))
        return r // (count_kv * count_tp) + outer[here] + inner * (inside[here] - outer[here])

    near = sorted(range(1, count), key=lambda r: (level(r), r % count_tp))
    levels = count_dp + count_kv - 1
    last = 5 + levels
    peers = sorted(range(count_tp, count, count_tp), key=level)[::-1]

    def gain_row(which, at, width):
        lines = width // 128
        first = at * lines
        return jnp.concatenate(
            [gains[which, pl.ds(first + i, 1), :] for i in range(lines)], axis=1
        )

    def load(hbm, vmem, index, pieces=1):
        step = hbm.shape[0] // pieces
        for i in range(pieces):
            pltpu.make_async_copy(
                hbm.at[pl.ds(i * step, step)], vmem.at[pl.ds(i * step, step)], load_sem.at[index]
            ).start()

    def loaded(vmem, index):
        pltpu.make_async_copy(vmem, vmem, load_sem.at[index]).wait()

    def remote(src, dst, send, recv, r, core=None):
        where = device(r)
        if core is not None:
            where["tp"] = core
        pltpu.make_async_remote_copy(
            src_ref=src, dst_ref=dst, send_sem=send_sem.at[0], recv_sem=recv_sem.at[recv],
            device_id=where, device_id_type=pl.DeviceIdType.MESH,
        ).start()

    def arrived(like, recv):
        pltpu.make_async_copy(like, like, recv_sem.at[recv]).wait()

    def sent(like, send):
        pltpu.make_async_copy(like, like, send_sem.at[0]).wait()

    barrier = pltpu.get_barrier_semaphore()

    def greet(r, core):
        where = device(r)
        where["tp"] = core
        pl.semaphore_signal(barrier, inc=1, device_id=where, device_id_type=pl.DeviceIdType.MESH)

    for r in peers:
        greet(r, lead)
    greet(0, tp ^ 1)
    for r in peers:
        pl.when(target(r)[1] != 0)(functools.partial(greet, r, 0))
    load(tokens, tok_v, 0)
    load(gain_mix, gain_raw.at[0], 0)
    gate_start = pl.multiple_of(block * feat, feat)
    pltpu.make_async_copy(w_gates.at[:, pl.ds(gate_start, feat)], wg_v, load_sem.at[0]).start()
    load(w_query, wq_v, 2, 4)
    load(lengths, len_s, 1)
    load(cache_igate, igate_v, 1)
    load(cache_fcum, fcum_v, 1)
    load(w_key, wk_v, 3, 2)
    load(w_value, wv_v, 3, 4)

    dot = functools.partial(jnp.dot, preferred_element_type=f32)
    loaded(tok_v, 0)
    loaded(gain_raw.at[0], 0)
    loaded(wg_v, 0)
    gains[0] = gain_raw[0].astype(f32)
    token = tok_v[...].astype(f32)
    scaled = (token * gain_row(0, block, feat)).astype(bf16)
    energy = jnp.sum(token * token, axis=1, keepdims=True)
    gate_part = lax.dot_general(
        scaled, wg_v[...], (((1,), (1,)), ((), ())), preferred_element_type=f32
    )
    gate_part = jnp.concatenate(
        [gate_part, jnp.zeros((rows, 128 - 2 * heads_total), f32)], axis=1
    )
    shifted = gate_part
    for c in range(1, count_tp):
        shifted = jnp.where(tp == c, pltpu.roll(gate_part, 128 - c * heads, 1), shifted)
    lane_all = lax.broadcasted_iota(jnp.int32, (rows, 128), 1)
    at_energy, at_max, at_anchor = 16, 32, 64
    shifted = jnp.where(lane_all == at_energy, energy, shifted)

    loaded(len_s, 1)
    loaded(igate_v, 1)
    loaded(fcum_v, 1)
    lane = lax.broadcasted_iota(jnp.int32, (seqs, 128), 1)
    row = lax.broadcasted_iota(jnp.int32, (seqs, block_len), 0)
    row_v = lax.broadcasted_iota(jnp.int32, (seqs, value_size), 0)
    length = jnp.zeros((seqs, block_len), jnp.int32)
    for s in range(seqs):
        length = jnp.where(row == s, len_s[s], length)
    position = kv * block_len + lax.broadcasted_iota(jnp.int32, (seqs, block_len), 1)
    live = position < length
    holding = position == length - 1
    exponents = []
    stats = jnp.full((seqs, 128), very_low, f32)
    for h in range(heads):
        fcum = fcum_v[h]
        exponent = jnp.where(live, igate_v[h] - fcum, very_low)
        exponents.append(exponent)
        top = jnp.max(exponent, axis=1, keepdims=True)
        anchor = jnp.max(jnp.where(holding, fcum, very_low), axis=1, keepdims=True)
        stats = jnp.where(lane == at_max + h, top, stats)
        stats = jnp.where(lane == at_anchor + h, anchor, stats)
    for a in range(count_dp):
        part = shifted[a * seqs : (a + 1) * seqs]
        small_src[a] = jnp.where(lane < at_max, part, stats)

    loaded(wq_v, 2)
    for s in range(seqs):
        span = pl.ds(s * block_len, block_len)
        pltpu.make_async_copy(cache_keys.at[s], keys_v.at[:, span, :], load_sem.at[4]).start()
    for s in range(seqs):
        span = pl.ds(s * block_len, block_len)
        pltpu.make_async_copy(cache_values.at[s], values_v.at[:, span, :], load_sem.at[5]).start()
    query = dot(scaled, wq_v[...])
    for a in range(count_dp):
        q_src[a] = query[a * seqs : (a + 1) * seqs].astype(bf16)
    def keys_and_values():
        loaded(wk_v, 3)
        loaded(wv_v, 3)
        joined = jnp.concatenate([dot(scaled, wk_v[...]), dot(scaled, wv_v[...])], axis=1)
        for i in range(rows):
            line = joined[i : i + 1]
            kv_src[i] = jnp.concatenate([line[:, :half_kv], line[:, half_kv:]], axis=0).astype(bf16)

    def send_query(small, query, r, core):
        n, to = slot(r) // count_tp, target(r)[0]
        remote(small.at[to], small_rx.at[n], 0, 0, r, core)
        remote(query.at[to], q_rx.at[n], 0, 1, r, core)

    def send_values(source, r, core):
        t = target(r)
        remote(source.at[t[0] * count_kv + t[1]], kv_rx.at[slot(r) // count_tp], 0, 2, r, core)

    early = kv == 0

    @pl.when(jnp.logical_and(early, follows))
    def _():
        pl.semaphore_wait(barrier, 1)
        remote(small_src, small_via, 0, last + 2, 1)
        remote(q_src, q_via, 0, last + 3, 1)
        keys_and_values()
        remote(kv_src, kv_via, 0, last + 4, 1)

    @pl.when(jnp.logical_and(early, leads))
    def _():
        keys_and_values()
        pl.semaphore_wait(barrier, count - 1)
        arrived(small_via, last + 2)
        arrived(q_via, last + 3)
        arrived(kv_via, last + 4)
        for r in peers:
            send_query(small_via, q_via, r, 0)
            send_values(kv_via, r, 0)
        for r in peers:
            send_query(small_src, q_src, r, lead)
            send_values(kv_src, r, lead)

    @pl.when(kv != 0)
    def _():
        pl.semaphore_wait(barrier, count - 1)
        for r in peers:
            send_query(small_src, q_src, r, tp)
        keys_and_values()
        for r in peers:
            send_values(kv_src, r, tp)

    @pl.when(follows)
    def _():
        remote(w_out, wo_v.at[tp], 7, last + 1, 0, lead)

    @pl.when(leads)
    def _():
        load(w_out, wo_v.at[lead], 6, 4)

    load(gain_ffn, gain_raw.at[1], 7)
    load(w_gate, wgate_v, 8, 8)
    load(w_up, wup_v, 8, 8)
    for j in range(count):
        pltpu.make_async_copy(
            w_down.at[:, pl.ds(j * out_block, out_block)], wdown_v.at[j], load_sem.at[9]
        ).start()

    loaded(keys_v, 4)
    for h in range(heads):
        keys_t[h] = keys_v[h].T

    arrived(small_rx.at[pl.ds(1, blocks - 1)], 0)
    arrived(q_rx.at[pl.ds(1, blocks - 1)], 1)
    small = small_src[dp]
    extreme = small
    for n in range(1, blocks):
        small += small_rx[n]
        if n < count_kv:
            extreme = jnp.maximum(extreme, small_rx[n])
    inv_norm = lax.rsqrt(small[:, at_energy : at_energy + 1] / model_width + epsilon)
    q_total = q_src[dp].astype(f32)
    for n in range(1, blocks):
        q_total += q_rx[n].astype(f32)
    query_new = (q_total * inv_norm).astype(bf16)
    founds = [
        dot(query_new[:, h * key_size : (h + 1) * key_size], keys_t[h]) for h in range(heads)
    ]
    gates_now = small * inv_norm
    log_forget = jnp.minimum(gates_now, 0.0) - jnp.log1p(jnp.exp(-jnp.abs(gates_now)))
    forget_here = pltpu.roll(log_forget, 128 - heads_total, 1)
    top_here = pltpu.roll(extreme, 128 - at_max, 1)
    carried = pltpu.roll(extreme, 128 - at_anchor, 1) + forget_here
    highest = jnp.maximum(carried + top_here, gates_now)
    offset = carried - highest
    own_weight = jnp.exp(gates_now - highest)
    weights = []
    for h in range(heads):
        power = jnp.where(live, exponents[h] + offset[:, h : h + 1], very_low)
        weights.append(jnp.where(live, jnp.exp(power), 0.0))

    inv_root = key_size ** (-0.5)
    probs, dens, nums = [], [], []
    for h in range(heads):
        found = founds[h]
        score = found[:, 0:block_len]
        for s in range(1, seqs):
            score = jnp.where(row == s, found[:, s * block_len : (s + 1) * block_len], score)
        product = weights[h] * (score * inv_root)
        dens.append(jnp.sum(product, axis=1, keepdims=True))
        probs.append(
            jnp.concatenate([jnp.where(row == s, product, 0.0) for s in range(seqs)], axis=1).astype(bf16)
        )
    loaded(values_v, 5)
    arrived(kv_rx.at[pl.ds(1, blocks - 1)], 2)
    for h in range(heads):
        nums.append(dot(probs[h], values_v[h]))
    kv_total = kv_src[block].astype(f32)
    for n in range(1, blocks):
        kv_total += kv_rx[n].astype(f32)
    kv_row = jnp.concatenate([kv_total[0:1], kv_total[1:2]], axis=1)
    kv_row = (jnp.broadcast_to(kv_row, (seqs, 2 * half_kv)) * inv_norm).astype(bf16).astype(f32)
    query_f32 = query_new.astype(f32)
    mine = lax.broadcasted_iota(jnp.int32, (seqs, 1), 0) == kv
    den_line = jnp.zeros((seqs, 128), f32)
    for h in range(heads):
        key_h = kv_row[:, h * key_size : (h + 1) * key_size]
        value_h = kv_row[:, width_q + h * value_size : width_q + (h + 1) * value_size]
        query_h = query_f32[:, h * key_size : (h + 1) * key_size]
        score = jnp.sum(query_h * key_h, axis=1, keepdims=True) * inv_root
        own = jnp.where(mine, own_weight[:, h : h + 1], 0.0)
        dens[h] += own * score
        nums[h] += (own * score.astype(bf16).astype(f32)) * value_h
        coarse = dens[h].astype(bf16).astype(f32)
        den_line = jnp.where(lane == h, coarse, den_line)
        den_line = jnp.where(lane == heads + h, dens[h] - coarse, den_line)
        span = pl.ds(h * value_size, value_size)
        part_src[:, span] = nums[h].astype(bf16)
        own_part[:, span] = nums[h]
    den_here = pl.ds(width_v, 128)
    part_src[:, den_here] = den_line.astype(bf16)
    own_part[:, den_here] = den_line
    for b in range(count_kv - 1, 0, -1):
        remote(part_src, part_rx.at[tp * count_kv + by_reach[b]], 3, 3, b * count_tp, lead)

    @pl.when(follows)
    def _():
        remote(part_src, part_rx.at[tp * count_kv], 3, 3, 0, lead)
        sent(part_rx.at[pl.ds(0, count_kv)], 3)
        sent(w_out, 7)

    @pl.when(leads)
    def _():
        arrived(part_rx.at[pl.ds(0, count_tp * count_kv - 1)], 3)
        for c in range(count_tp):
            def summed(span):
                held = [part_rx[c * count_kv + b, :, span].astype(f32) for b in range(1, count_kv)]
                held.append(own_part[:, span] if c == lead else part_rx[c * count_kv, :, span].astype(f32))
                return functools.reduce(jnp.add, held)

            tail = summed(den_here)
            for h in range(heads):
                den = tail[:, h : h + 1] + tail[:, heads + h : heads + h + 1]
                num = summed(pl.ds(h * value_size, value_size))
                span = pl.ds(c * width_v + h * value_size, value_size)
                heads_rx[dp, :, span] = (num / jnp.maximum(jnp.abs(den), 1.0)).astype(bf16)
        for a in range(1, count_dp):
            remote(heads_rx.at[dp], heads_rx.at[dp], 4, 4, a * count_kv * count_tp)
        loaded(wo_v.at[lead], 6)
        arrived(wo_v.at[pl.ds(0, count_tp - 1)], last + 1)
        arrived(heads_rx.at[pl.ds(0, count_dp - 1)], 4)
        lines = jnp.concatenate([heads_rx[a].astype(f32) for a in range(count_dp)], axis=0).astype(bf16)
        attended = jnp.concatenate([dot(lines, wo_v[c]) for c in range(count_tp)], axis=1)
        resid_rx[block] = (tok_v[...].astype(f32) + attended).astype(bf16)
        for r in near[::-1]:
            remote(resid_rx.at[block], resid_rx.at[block], 5, 5 + jnp.minimum(level_there(r), levels - 2), r)
        sent(part_rx.at[pl.ds(0, count_kv - 1)], 3)
        sent(heads_rx.at[pl.ds(0, count_dp - 1)], 4)

    loaded(gain_raw.at[1], 7)
    gains[1] = gain_raw[1].astype(f32)
    loaded(wgate_v, 8)
    loaded(wup_v, 8)
    gate_act = up_act = square = 0.0

    @pl.when(follows)
    def _():
        arrived(resid_rx.at[pl.ds(0, 1)], 5)

    for i in range(levels - 1):
        group = [r for r in range(0, count, count_tp) if min(level(r), levels - 2) == i]
        if i:
            arrived(resid_rx.at[pl.ds(0, len(group))], 5 + i)
        for r in group:
            at = place(r) // count_tp
            piece = resid_rx[at].astype(f32)
            square += jnp.sum(piece * piece, axis=1, keepdims=True)
            piece = (piece * gain_row(1, at, feat)).astype(bf16)
            span = pl.ds(pl.multiple_of(at * feat, feat), feat)
            gate_act += dot(piece, wgate_v[span, :])
            up_act += dot(piece, wup_v[span, :])
        if i < 1:
            acc_v[0] = gate_act
            acc_v[1] = up_act
            gate_act, up_act = acc_v[0], acc_v[1]
    inv_ffn = lax.rsqrt(square / model_width + epsilon)
    gate_act = gate_act * inv_ffn
    up_act = up_act * inv_ffn
    hidden = (gate_act / (1.0 + jnp.exp(-gate_act)) * up_act).astype(bf16)
    loaded(wdown_v, 9)
    def deliver(pair, results):
        for r, result in zip(pair, results):
            down_src[r] = result.astype(bf16)
        for r in pair:
            remote(down_src.at[r], down_rx.at[slot(r)], 6, last, r)

    order = near[::-1]
    pending = None
    for first in range(0, count - 1, 2):
        pair = order[first : first + 2]
        results = [dot(hidden, wdown_v[place(r)]) for r in pair]
        if pending:
            deliver(*pending)
        pending = (pair, results)
    total = dot(hidden, wdown_v[me])
    deliver(*pending)
    residual = resid_rx[block, :, pl.ds(pl.multiple_of(tp * out_block, out_block), out_block)]
    total += residual.astype(f32)

    def first_sent():
        sent(small_rx.at[pl.ds(1, blocks - 1)], 0)
        sent(q_rx.at[pl.ds(1, blocks - 1)], 0)
        sent(kv_rx.at[pl.ds(1, blocks - 1)], 0)

    @pl.when(jnp.logical_and(early, follows))
    def _():
        sent(small_src, 0)
        sent(q_src, 0)
        sent(kv_src, 0)

    pl.when(jnp.logical_and(early, leads))(first_sent)
    pl.when(jnp.logical_or(kv != 0, leads))(first_sent)

    @pl.when(leads)
    def _():
        for _ in range(count_tp):
            sent(resid_rx.at[pl.ds(0, blocks - 1)], 5)
        sent(resid_rx.at[pl.ds(0, count_tp - 1)], 5)

    arrived(down_rx.at[pl.ds(1, count - 1)], last)
    for r in near:
        total += down_rx[r].astype(f32)
    out_ref[...] = total.astype(bf16)
    sent(down_rx.at[pl.ds(1, count - 1)], 6)


def fused(
    tokens, lengths, cache_keys, cache_values, cache_igate, cache_fcum, gain_mix,
    w_query, w_key, w_value, w_gates, w_out, gain_ffn, w_gate, w_up, w_down,
):
    sizes = tuple(lax.axis_size(name) for name in ("dp", "kv", "tp"))
    count = sizes[0] * sizes[1] * sizes[2]
    blocks = sizes[0] * sizes[1]
    f32, bf16 = jnp.float32, jnp.bfloat16
    rows, feat = tokens.shape
    seqs, block_len, heads, key_size = cache_keys.shape
    value_size = cache_values.shape[3]
    out_block = w_out.shape[1]
    half_kv = heads * (key_size + value_size) // 2
    width_v = heads * value_size
    hbm = pl.BlockSpec(memory_space=pl.ANY)
    vmem = pl.BlockSpec(memory_space=pltpu.VMEM)
    dma = pltpu.SemaphoreType.DMA
    scratch = [
        pltpu.SMEM((seqs,), jnp.int32),
        pltpu.VMEM(tokens.shape, bf16),
        pltpu.VMEM((heads, seqs, block_len), f32),
        pltpu.VMEM((heads, seqs, block_len), f32),
        pltpu.VMEM((2, blocks * feat // 128, 128), bf16),
        pltpu.VMEM(w_query.shape, bf16),
        pltpu.VMEM(w_key.shape, bf16),
        pltpu.VMEM(w_value.shape, bf16),
        pltpu.VMEM((w_gates.shape[1], feat), bf16),
        pltpu.VMEM((sizes[2],) + w_out.shape, bf16),
        pltpu.VMEM(w_gate.shape, bf16),
        pltpu.VMEM(w_up.shape, bf16),
        pltpu.VMEM((count, w_down.shape[0], out_block), bf16),
        pltpu.VMEM((heads, seqs * block_len, key_size), bf16),
        pltpu.VMEM((heads, seqs * block_len, value_size), bf16),
        pltpu.VMEM((heads, key_size, seqs * block_len), bf16),
        pltpu.VMEM((sizes[0], seqs, heads * key_size), bf16),
        pltpu.VMEM((rows, 2, half_kv), bf16),
        pltpu.VMEM((sizes[0], seqs, 128), f32),
        pltpu.VMEM((blocks, seqs, heads * key_size), bf16),
        pltpu.VMEM((blocks, 2, half_kv), bf16),
        pltpu.VMEM((blocks, seqs, 128), f32),
        pltpu.VMEM((sizes[0], seqs, heads * key_size), bf16),
        pltpu.VMEM((rows, 2, half_kv), bf16),
        pltpu.VMEM((sizes[0], seqs, 128), f32),
        pltpu.VMEM((2, rows, w_gate.shape[1]), f32),
        pltpu.VMEM((seqs, width_v + 128), f32),
        pltpu.VMEM((seqs, width_v + 128), bf16),
        pltpu.VMEM((sizes[2] * sizes[1], seqs, width_v + 128), bf16),
        pltpu.VMEM((sizes[0], seqs, sizes[2] * width_v), bf16),
        pltpu.VMEM((blocks, rows, feat), bf16),
        pltpu.VMEM((count, rows, out_block), bf16),
        pltpu.VMEM((count, rows, out_block), bf16),
        pltpu.VMEM((2, blocks * feat // 128, 128), f32),
        dma((10,)),
        dma((1,)),
        dma((5 + sizes[0] + sizes[1] - 1 + 5,)),
    ]
    operands = (
        lengths, tokens, cache_igate.swapaxes(0, 1), cache_fcum.swapaxes(0, 1),
        gain_mix.reshape(-1, 128), gain_ffn.reshape(-1, 128),
        cache_keys.swapaxes(1, 2), cache_values.swapaxes(1, 2),
        w_query, w_key, w_value, w_gates.T, w_out, w_gate, w_up, w_down,
    )
    return pl.pallas_call(
        functools.partial(fused_kernel, sizes),
        out_shape=pltpu.VMEM((rows, out_block), bf16),
        in_specs=[hbm] * len(operands),
        out_specs=vmem,
        scratch_shapes=scratch,
        compiler_params=pltpu.CompilerParams(
            collective_id=0, has_side_effects=True, vmem_limit_bytes=40 * 1024 * 1024
        ),
    )(*[pltpu.with_memory_space_constraint(x, pltpu.HBM) for x in operands])


def fits_kernel(tokens, cache_keys, w_out, w_gate):
    return (
        cache_keys.shape[0] == lax.axis_size("kv")
        and all(n in (2, 4) for n in map(lax.axis_size, ("dp", "kv")))
        and lax.axis_size("tp") == 2
        and cache_keys.shape[2] <= 4
        and tokens.shape[1] % 128 == 0
        and w_out.shape[1] % 128 == 0
        and w_gate.shape[1] % 128 == 0
    )


def layer(*args):
    if fits_kernel(args[0], args[2], args[11], args[13]):
        return fused(*args)
    return per_device(*args)


def solution(mesh):
    in_specs = (
        P("grp", ("dp", "kv")),
        P(("grp", "dp")),
        P(("grp", "dp"), "kv", "tp", None),
        P(("grp", "dp"), "kv", "tp", None),
        P(("grp", "dp"), "tp", "kv"),
        P(("grp", "dp"), "tp", "kv"),
        P(),
        P(("dp", "kv"), "tp"),
        P(("dp", "kv"), "tp"),
        P(("dp", "kv"), "tp"),
        P(),
        P(None, ("dp", "kv", "tp")),
        P(),
        P(None, ("dp", "kv", "tp")),
        P(None, ("dp", "kv", "tp")),
        P(("dp", "kv", "tp"), None),
    )
    out_specs = P("grp", ("dp", "kv", "tp"))
    return jax.shard_map(
        layer, mesh=mesh, in_specs=in_specs, out_specs=out_specs, check_vma=False
    )
```

```python
import functools

import jax
import jax.numpy as jnp
from jax import lax
from jax.experimental import pallas as pl
from jax.experimental.pallas import tpu as pltpu
from jax.sharding import PartitionSpec as P

epsilon = 1e-06
very_low = -1e30


def combined_all(value, axis, join):
    pieces = jax.tree.map(lambda part: lax.all_gather(part, axis), value)
    head = jax.tree.map(lambda part: part[0], pieces)
    tail = jax.tree.map(lambda part: part[1:], pieces)
    total, _ = lax.scan(lambda total, piece: (join(total, piece), None), head, tail)
    return total


def merge_partial(first_part, second_part):
    max_first, den_first, num_first, anchor_first = first_part
    max_second, den_second, num_second, anchor_second = second_part
    highest = jnp.maximum(max_first, max_second)
    scale_first = jnp.exp(max_first - highest)
    scale_second = jnp.exp(max_second - highest)
    denominator = scale_first * den_first + scale_second * den_second
    numerator = scale_first[..., None] * num_first + scale_second[..., None] * num_second
    return (highest, denominator, numerator, jnp.maximum(anchor_first, anchor_second))


def per_device(
    tokens,
    lengths,
    cache_keys,
    cache_values,
    cache_igate,
    cache_fcum,
    gain_mix,
    w_query,
    w_key,
    w_value,
    w_gates,
    w_out,
    gain_ffn,
    w_gate,
    w_up,
    w_down,
):
    count_dp = lax.axis_size("dp")
    count_kv = lax.axis_size("kv")
    count_tp = lax.axis_size("tp")
    index_dp = lax.axis_index("dp")
    index_kv = lax.axis_index("kv")
    index_tp = lax.axis_index("tp")
    row_count, feat_block = tokens.shape
    seq_count, block_len, head_local, key_dimension = cache_keys.shape
    value_size = cache_values.shape[3]
    model_width = gain_mix.shape[0]
    heads_total = w_gates.shape[1] // 2
    out_block = w_out.shape[1]
    col_start = (index_dp * count_kv + index_kv) * feat_block
    token_f32 = tokens.astype(jnp.float32)
    gain_part = lax.dynamic_slice_in_dim(gain_mix, col_start, feat_block, 0).astype(jnp.float32)
    scaled = (token_f32 * gain_part[None, :]).astype(jnp.bfloat16)
    energy = jnp.sum(token_f32 * token_f32, axis=1)
    joined = jnp.concatenate(
        [
            jnp.dot(scaled, w_query, preferred_element_type=jnp.float32),
            jnp.dot(scaled, w_key, preferred_element_type=jnp.float32),
            jnp.dot(scaled, w_value, preferred_element_type=jnp.float32),
        ],
        axis=1,
    )
    gate_rows = lax.dynamic_slice_in_dim(w_gates, col_start, feat_block, 0).reshape(
        feat_block, 2, heads_total
    )
    gate_cols = lax.dynamic_slice_in_dim(gate_rows, index_tp * head_local, head_local, 2).reshape(
        feat_block, 2 * head_local
    )
    gate_part = jnp.dot(scaled, gate_cols, preferred_element_type=jnp.float32)
    joined_part, gate_rowsum, energy_part = (
        lax.psum_scatter(joined, "dp", scatter_dimension=0, tiled=True),
        lax.psum_scatter(gate_part, "dp", scatter_dimension=0, tiled=True),
        lax.psum_scatter(energy, "dp", scatter_dimension=0, tiled=True),
    )
    joined_own, gate_own, energy_own = lax.psum((joined_part, gate_rowsum, energy_part), "kv")
    inv_norm = lax.rsqrt(energy_own / model_width + epsilon)[:, None]
    width_qk = head_local * key_dimension
    query_new = (
        (joined_own[:, :width_qk] * inv_norm)
        .astype(jnp.bfloat16)
        .reshape(seq_count, head_local, key_dimension)
    )
    new_key = (
        (joined_own[:, width_qk : 2 * width_qk] * inv_norm)
        .astype(jnp.bfloat16)
        .reshape(seq_count, head_local, key_dimension)
    )
    new_value = (
        (joined_own[:, 2 * width_qk :] * inv_norm)
        .astype(jnp.bfloat16)
        .reshape(seq_count, head_local, value_size)
    )
    gates_now = gate_own * inv_norm
    in_gate = gates_now[:, :head_local]
    log_forget = jax.nn.log_sigmoid(gates_now[:, head_local:])
    inv_root = key_dimension ** (-0.5)
    scores = (
        jnp.einsum("shk,sphk->shp", query_new, cache_keys, preferred_element_type=jnp.float32)
        * inv_root
    )
    positions = index_kv * block_len + jnp.arange(block_len, dtype=jnp.int32)
    is_live = positions[None, None, :] < lengths[:, None, None]
    exponent = jnp.where(is_live, cache_igate - cache_fcum, very_low)
    block_max = jnp.max(exponent, axis=2)
    weight = jnp.where(is_live, jnp.exp(exponent - block_max[..., None]), 0.0)
    product = weight * scores
    block_den = jnp.sum(product, axis=2)
    block_num = jnp.einsum(
        "shp,sphv->shv",
        product.astype(jnp.bfloat16),
        cache_values,
        preferred_element_type=jnp.float32,
    )
    holding = positions[None, None, :] == (lengths - 1)[:, None, None]
    anchor = jnp.max(jnp.where(holding, cache_fcum, very_low), axis=2)
    cache_max, cache_den, cache_num, anchor_all = combined_all(
        (block_max, block_den, block_num, anchor), "kv", merge_partial
    )
    own_score = (
        jnp.sum(query_new.astype(jnp.float32) * new_key.astype(jnp.float32), axis=2) * inv_root
    )
    own_prob = lax.optimization_barrier(own_score.astype(jnp.bfloat16)).astype(jnp.float32)
    own_num = own_prob[..., None] * new_value.astype(jnp.float32)
    carried = anchor_all + log_forget
    highest = jnp.maximum(carried + cache_max, in_gate)
    weight_cache = jnp.exp(carried + cache_max - highest)
    weight_own = jnp.exp(in_gate - highest)
    denominator = weight_cache * cache_den + weight_own * own_score
    numerator = weight_cache[..., None] * cache_num + weight_own[..., None] * own_num
    heads_out = (numerator / jnp.maximum(jnp.abs(denominator), 1.0)[..., None]).astype(jnp.bfloat16)
    heads_out = heads_out.reshape(seq_count, head_local * value_size)
    gathered = lax.all_gather(heads_out[None], ("dp", "tp"), axis=0, tiled=True)
    gathered = gathered.reshape(count_dp, count_tp, seq_count, head_local * value_size)
    out_weight = w_out.reshape(count_tp, head_local * value_size, out_block)
    attended = jnp.einsum(
        "atsk,tkc->asc", gathered, out_weight, preferred_element_type=jnp.float32
    ).reshape(row_count, out_block)
    own_cols = lax.dynamic_slice_in_dim(token_f32, index_tp * out_block, out_block, 1)
    residual = (own_cols + attended).astype(jnp.bfloat16)
    full_rows = lax.all_gather(residual, ("dp", "kv", "tp"), axis=1, tiled=True)
    full_f32 = full_rows.astype(jnp.float32)
    inv_norm_ffn = lax.rsqrt(jnp.mean(full_f32 * full_f32, axis=1, keepdims=True) + epsilon)
    normed = (full_f32 * inv_norm_ffn * gain_ffn.astype(jnp.float32)[None, :]).astype(jnp.bfloat16)
    gate_act = jnp.dot(normed, w_gate, preferred_element_type=jnp.float32)
    up_act = jnp.dot(normed, w_up, preferred_element_type=jnp.float32)
    hidden = (jax.nn.silu(gate_act) * up_act).astype(jnp.bfloat16)
    summed = lax.psum_scatter(
        lax.dot_general(
            w_down, hidden, (((0,), (1,)), ((), ())), preferred_element_type=jnp.float32
        ),
        ("dp", "kv", "tp"),
        scatter_dimension=0,
        tiled=True,
    )
    return (residual.astype(jnp.float32) + summed.T).astype(jnp.bfloat16)


def fused_kernel(
    sizes, lengths, tokens, cache_igate, cache_fcum, gain_mix, gain_ffn,
    cache_keys, cache_values, w_query, w_key, w_value, w_gates, w_out, w_gate, w_up, w_down,
    out_ref,
    len_s, tok_v, igate_v, fcum_v, gain_raw,
    wq_v, wk_v, wv_v, wg_v, wo_v, wgate_v, wup_v, wdown_v,
    keys_v, values_v,
    keys_t, q_src, kv_src, small_src, q_rx, kv_rx, small_rx, q_via, kv_via, small_via,
    acc_v, own_part, part_src, part_rx, heads_rx, resid_rx, down_src, down_rx, gains,
    load_sem, send_sem, recv_sem,
):
    count_dp, count_kv, count_tp = sizes
    count = count_dp * count_kv * count_tp
    blocks = count_dp * count_kv
    dp, kv, tp = lax.axis_index("dp"), lax.axis_index("kv"), lax.axis_index("tp")
    f32, bf16 = jnp.float32, jnp.bfloat16
    seqs, heads, block_len, key_size = cache_keys.shape
    value_size = cache_values.shape[3]
    rows, feat = tokens.shape
    width_q = heads * key_size
    width_v = heads * value_size
    half_kv = (width_q + width_v) // 2
    out_block = out_ref.shape[1]
    model_width = feat * blocks
    heads_total = heads * count_tp
    block = dp * count_kv + kv
    me = block * count_tp + tp
    lead = count_tp - 1
    leads, follows = tp == lead, tp != lead

    inner = (kv ^ (kv >> 1)) & 1
    by_reach = {i: i for i in range(count_kv)}
    if count_kv == 4:
        by_reach = {i: i + inner * (b - i) for i, b in enumerate((0, 3, 1, 2))}

    def step(r):
        return r // (count_kv * count_tp), by_reach[(r // count_tp) % count_kv], r % count_tp

    def target(r):
        a, b, c = step(r)
        return dp ^ a, kv ^ b, tp ^ c

    def place(r):
        t = target(r)
        return (t[0] * count_kv + t[1]) * count_tp + t[2]

    def slot(r):
        a, b, c = step(r)
        return (a * count_kv + b) * count_tp + c

    def device(r):
        t = target(r)
        return {"dp": t[0], "kv": t[1], "tp": t[2]}

    def level(r):
        return r // (count_kv * count_tp) + (r // count_tp) % count_kv

    def level_there(r):
        here = (r // count_tp) % count_kv
        if count_kv != 4:
            return level(r)
        outer, inside = ((0, 2, 3, 3), (0, 1, 1, 2))
        return r // (count_kv * count_tp) + outer[here] + inner * (inside[here] - outer[here])

    near = sorted(range(1, count), key=lambda r: (level(r), r % count_tp))
    levels = count_dp + count_kv - 1
    last = 5 + levels
    peers = sorted(range(count_tp, count, count_tp), key=level)[::-1]

    def gain_row(which, at, width):
        lines = width // 128
        first = at * lines
        return jnp.concatenate(
            [gains[which, pl.ds(first + i, 1), :] for i in range(lines)], axis=1
        )

    def load(hbm, vmem, index, pieces=1):
        step = hbm.shape[0] // pieces
        for i in range(pieces):
            pltpu.make_async_copy(
                hbm.at[pl.ds(i * step, step)], vmem.at[pl.ds(i * step, step)], load_sem.at[index]
            ).start()

    def loaded(vmem, index):
        pltpu.make_async_copy(vmem, vmem, load_sem.at[index]).wait()

    def remote(src, dst, send, recv, r, core=None):
        where = device(r)
        if core is not None:
            where["tp"] = core
        pltpu.make_async_remote_copy(
            src_ref=src, dst_ref=dst, send_sem=send_sem.at[0], recv_sem=recv_sem.at[recv],
            device_id=where, device_id_type=pl.DeviceIdType.MESH,
        ).start()

    def arrived(like, recv):
        pltpu.make_async_copy(like, like, recv_sem.at[recv]).wait()

    def sent(like, send):
        pltpu.make_async_copy(like, like, send_sem.at[0]).wait()

    barrier = pltpu.get_barrier_semaphore()

    def greet(r, core):
        where = device(r)
        where["tp"] = core
        pl.semaphore_signal(barrier, inc=1, device_id=where, device_id_type=pl.DeviceIdType.MESH)

    for r in peers:
        greet(r, lead)
    greet(0, tp ^ 1)
    for r in peers:
        pl.when(target(r)[1] != 0)(functools.partial(greet, r, 0))
    load(tokens, tok_v, 0)
    load(gain_mix, gain_raw.at[0], 0)
    gate_start = pl.multiple_of(block * feat, feat)
    pltpu.make_async_copy(w_gates.at[:, pl.ds(gate_start, feat)], wg_v, load_sem.at[0]).start()
    load(w_query, wq_v, 2, 4)
    load(lengths, len_s, 1)
    load(cache_igate, igate_v, 1)
    load(cache_fcum, fcum_v, 1)
    load(w_key, wk_v, 3, 2)
    load(w_value, wv_v, 3, 4)

    dot = functools.partial(jnp.dot, preferred_element_type=f32)
    loaded(tok_v, 0)
    loaded(gain_raw.at[0], 0)
    loaded(wg_v, 0)
    gains[0] = gain_raw[0].astype(f32)
    token = tok_v[...].astype(f32)
    scaled = (token * gain_row(0, block, feat)).astype(bf16)
    energy = jnp.sum(token * token, axis=1, keepdims=True)
    gate_part = lax.dot_general(
        scaled, wg_v[...], (((1,), (1,)), ((), ())), preferred_element_type=f32
    )
    gate_part = jnp.concatenate(
        [gate_part, jnp.zeros((rows, 128 - 2 * heads_total), f32)], axis=1
    )
    shifted = gate_part
    for c in range(1, count_tp):
        shifted = jnp.where(tp == c, pltpu.roll(gate_part, 128 - c * heads, 1), shifted)
    lane_all = lax.broadcasted_iota(jnp.int32, (rows, 128), 1)
    lanes_each = 128 // seqs
    at_stat = lanes_each // 2
    at_energy = 2 * heads_total
    shifted = jnp.where(lane_all == at_energy, energy, shifted)

    loaded(len_s, 1)
    loaded(igate_v, 1)
    loaded(fcum_v, 1)
    lane = lax.broadcasted_iota(jnp.int32, (seqs, 128), 1)
    row = lax.broadcasted_iota(jnp.int32, (seqs, block_len), 0)
    row_v = lax.broadcasted_iota(jnp.int32, (seqs, value_size), 0)
    length = jnp.zeros((seqs, block_len), jnp.int32)
    for s in range(seqs):
        length = jnp.where(row == s, len_s[s], length)
    position = kv * block_len + lax.broadcasted_iota(jnp.int32, (seqs, block_len), 1)
    live = position < length
    holding = position == length - 1
    exponents = []
    stats = jnp.full((seqs, 128), very_low, f32)
    for h in range(heads):
        fcum = fcum_v[h]
        exponent = jnp.where(live, igate_v[h] - fcum, very_low)
        exponents.append(exponent)
        top = jnp.max(exponent, axis=1, keepdims=True)
        anchor = jnp.max(jnp.where(holding, fcum, very_low), axis=1, keepdims=True)
        stats = jnp.where(lane == at_stat + h, top, stats)
        stats = jnp.where(lane == at_stat + heads_total + h, anchor, stats)
    for a in range(count_dp):
        part = shifted[a * seqs : (a + 1) * seqs]
        part = jnp.where(lane < at_stat, part, stats)
        packed = jnp.where(row == 0, part, 0.0)
        for s in range(1, seqs):
            packed = jnp.where(row == s, pltpu.roll(part, s * lanes_each, 1), packed)
        own_lanes = jnp.logical_and(lane >= row * lanes_each, lane < (row + 1) * lanes_each)
        small_src[a] = jnp.sum(jnp.where(own_lanes, packed, 0.0), axis=0, keepdims=True)

    loaded(wq_v, 2)
    for s in range(seqs):
        span = pl.ds(s * block_len, block_len)
        pltpu.make_async_copy(cache_keys.at[s], keys_v.at[:, span, :], load_sem.at[4]).start()
    for s in range(seqs):
        span = pl.ds(s * block_len, block_len)
        pltpu.make_async_copy(cache_values.at[s], values_v.at[:, span, :], load_sem.at[5]).start()
    query = dot(scaled, wq_v[...])
    for a in range(count_dp):
        q_src[a] = query[a * seqs : (a + 1) * seqs].astype(bf16)
    def keys_and_values():
        loaded(wk_v, 3)
        loaded(wv_v, 3)
        joined = jnp.concatenate([dot(scaled, wk_v[...]), dot(scaled, wv_v[...])], axis=1)
        for i in range(rows):
            line = joined[i : i + 1]
            kv_src[i] = jnp.concatenate([line[:, :half_kv], line[:, half_kv:]], axis=0).astype(bf16)

    def send_query(small, query, r, core):
        n, to = slot(r) // count_tp, target(r)[0]
        remote(small.at[to], small_rx.at[n], 0, 0, r, core)
        remote(query.at[to], q_rx.at[n], 0, 1, r, core)

    def send_values(source, r, core):
        t = target(r)
        remote(source.at[t[0] * count_kv + t[1]], kv_rx.at[slot(r) // count_tp], 0, 2, r, core)

    early = kv == 0

    @pl.when(jnp.logical_and(early, follows))
    def _():
        pl.semaphore_wait(barrier, 1)
        remote(small_src, small_via, 0, last + 2, 1)
        remote(q_src, q_via, 0, last + 3, 1)
        keys_and_values()
        remote(kv_src, kv_via, 0, last + 4, 1)

    @pl.when(jnp.logical_and(early, leads))
    def _():
        keys_and_values()
        pl.semaphore_wait(barrier, count - 1)
        arrived(small_via, last + 2)
        arrived(q_via, last + 3)
        arrived(kv_via, last + 4)
        for r in peers:
            send_query(small_via, q_via, r, 0)
            send_query(small_src, q_src, r, lead)
            send_values(kv_via, r, 0)
            send_values(kv_src, r, lead)

    @pl.when(kv != 0)
    def _():
        pl.semaphore_wait(barrier, count - 1)
        for r in peers:
            send_query(small_src, q_src, r, tp)
        keys_and_values()
        for r in peers:
            send_values(kv_src, r, tp)

    @pl.when(follows)
    def _():
        remote(w_out, wo_v.at[tp], 7, last + 1, 0, lead)

    @pl.when(leads)
    def _():
        load(w_out, wo_v.at[lead], 6, 4)

    load(gain_ffn, gain_raw.at[1], 7)
    load(w_gate, wgate_v, 8, 8)
    load(w_up, wup_v, 8, 8)
    for j in range(count):
        pltpu.make_async_copy(
            w_down.at[:, pl.ds(j * out_block, out_block)], wdown_v.at[j], load_sem.at[9]
        ).start()

    loaded(keys_v, 4)
    for h in range(heads):
        keys_t[h] = keys_v[h].T

    arrived(small_rx.at[pl.ds(1, blocks - 1)], 0)
    arrived(q_rx.at[pl.ds(1, blocks - 1)], 1)
    small = small_src[dp]
    extreme = small
    for n in range(1, blocks):
        small += small_rx[n]
        if n < count_kv:
            extreme = jnp.maximum(extreme, small_rx[n])
    first = lax.broadcasted_iota(jnp.int32, (1, 128), 1) % lanes_each < at_stat
    spread = jnp.broadcast_to(jnp.where(first, small, extreme), (seqs, 128))
    small = spread
    for s in range(1, seqs):
        small = jnp.where(row == s, pltpu.roll(spread, 128 - s * lanes_each, 1), small)
    inv_norm = lax.rsqrt(small[:, at_energy : at_energy + 1] / model_width + epsilon)
    q_total = q_src[dp].astype(f32)
    for n in range(1, blocks):
        q_total += q_rx[n].astype(f32)
    query_new = (q_total * inv_norm).astype(bf16)
    founds = [
        dot(query_new[:, h * key_size : (h + 1) * key_size], keys_t[h]) for h in range(heads)
    ]
    gates_now = small * inv_norm
    log_forget = jnp.minimum(gates_now, 0.0) - jnp.log1p(jnp.exp(-jnp.abs(gates_now)))
    forget_here = pltpu.roll(log_forget, 128 - heads_total, 1)
    top_here = pltpu.roll(small, 128 - at_stat, 1)
    carried = pltpu.roll(small, 128 - at_stat - heads_total, 1) + forget_here
    highest = jnp.maximum(carried + top_here, gates_now)
    offset = carried - highest
    own_weight = jnp.exp(gates_now - highest)
    weights = []
    for h in range(heads):
        power = jnp.where(live, exponents[h] + offset[:, h : h + 1], very_low)
        weights.append(jnp.where(live, jnp.exp(power), 0.0))

    inv_root = key_size ** (-0.5)
    probs, dens, nums = [], [], []
    for h in range(heads):
        found = founds[h]
        score = found[:, 0:block_len]
        for s in range(1, seqs):
            score = jnp.where(row == s, found[:, s * block_len : (s + 1) * block_len], score)
        product = weights[h] * (score * inv_root)
        dens.append(jnp.sum(product, axis=1, keepdims=True))
        probs.append(
            jnp.concatenate([jnp.where(row == s, product, 0.0) for s in range(seqs)], axis=1).astype(bf16)
        )
    loaded(values_v, 5)
    arrived(kv_rx.at[pl.ds(1, blocks - 1)], 2)
    for h in range(heads):
        nums.append(dot(probs[h], values_v[h]))
    kv_total = kv_src[block].astype(f32)
    for n in range(1, blocks):
        kv_total += kv_rx[n].astype(f32)
    kv_row = jnp.concatenate([kv_total[0:1], kv_total[1:2]], axis=1)
    kv_row = (jnp.broadcast_to(kv_row, (seqs, 2 * half_kv)) * inv_norm).astype(bf16).astype(f32)
    query_f32 = query_new.astype(f32)
    mine = lax.broadcasted_iota(jnp.int32, (seqs, 1), 0) == kv
    den_line = jnp.zeros((seqs, 128), f32)
    for h in range(heads):
        key_h = kv_row[:, h * key_size : (h + 1) * key_size]
        value_h = kv_row[:, width_q + h * value_size : width_q + (h + 1) * value_size]
        query_h = query_f32[:, h * key_size : (h + 1) * key_size]
        score = jnp.sum(query_h * key_h, axis=1, keepdims=True) * inv_root
        own = jnp.where(mine, own_weight[:, h : h + 1], 0.0)
        dens[h] += own * score
        nums[h] += (own * score.astype(bf16).astype(f32)) * value_h
        coarse = dens[h].astype(bf16).astype(f32)
        den_line = jnp.where(lane == h, coarse, den_line)
        den_line = jnp.where(lane == heads + h, dens[h] - coarse, den_line)
        span = pl.ds(h * value_size, value_size)
        part_src[:, span] = nums[h].astype(bf16)
        own_part[:, span] = nums[h]
    den_here = pl.ds(width_v, 128)
    part_src[:, den_here] = den_line.astype(bf16)
    own_part[:, den_here] = den_line
    for b in range(count_kv - 1, 0, -1):
        remote(part_src, part_rx.at[tp * count_kv + by_reach[b]], 3, 3, b * count_tp, lead)

    @pl.when(follows)
    def _():
        remote(part_src, part_rx.at[tp * count_kv], 3, 3, 0, lead)
        sent(part_rx.at[pl.ds(0, count_kv)], 3)
        sent(w_out, 7)

    @pl.when(leads)
    def _():
        arrived(part_rx.at[pl.ds(0, count_tp * count_kv - 1)], 3)
        for c in range(count_tp):
            def summed(span):
                held = [part_rx[c * count_kv + b, :, span].astype(f32) for b in range(1, count_kv)]
                held.append(own_part[:, span] if c == lead else part_rx[c * count_kv, :, span].astype(f32))
                return functools.reduce(jnp.add, held)

            tail = summed(den_here)
            for h in range(heads):
                den = tail[:, h : h + 1] + tail[:, heads + h : heads + h + 1]
                num = summed(pl.ds(h * value_size, value_size))
                span = pl.ds(c * width_v + h * value_size, value_size)
                heads_rx[dp, :, span] = (num / jnp.maximum(jnp.abs(den), 1.0)).astype(bf16)
        for a in range(1, count_dp):
            remote(heads_rx.at[dp], heads_rx.at[dp], 4, 4, a * count_kv * count_tp)
        loaded(wo_v.at[lead], 6)
        arrived(wo_v.at[pl.ds(0, count_tp - 1)], last + 1)
        arrived(heads_rx.at[pl.ds(0, count_dp - 1)], 4)
        lines = jnp.concatenate([heads_rx[a].astype(f32) for a in range(count_dp)], axis=0).astype(bf16)
        attended = jnp.concatenate([dot(lines, wo_v[c]) for c in range(count_tp)], axis=1)
        resid_rx[block] = (tok_v[...].astype(f32) + attended).astype(bf16)
        for r in near[::-1]:
            remote(resid_rx.at[block], resid_rx.at[block], 5, 5 + jnp.minimum(level_there(r), levels - 2), r)
        sent(part_rx.at[pl.ds(0, count_kv - 1)], 3)
        sent(heads_rx.at[pl.ds(0, count_dp - 1)], 4)

    loaded(gain_raw.at[1], 7)
    gains[1] = gain_raw[1].astype(f32)
    loaded(wgate_v, 8)
    loaded(wup_v, 8)
    gate_act = up_act = square = 0.0

    @pl.when(follows)
    def _():
        arrived(resid_rx.at[pl.ds(0, 1)], 5)

    for i in range(levels - 1):
        group = [r for r in range(0, count, count_tp) if min(level(r), levels - 2) == i]
        if i:
            arrived(resid_rx.at[pl.ds(0, len(group))], 5 + i)
        for r in group:
            at = place(r) // count_tp
            piece = resid_rx[at].astype(f32)
            square += jnp.sum(piece * piece, axis=1, keepdims=True)
            piece = (piece * gain_row(1, at, feat)).astype(bf16)
            span = pl.ds(pl.multiple_of(at * feat, feat), feat)
            gate_act += dot(piece, wgate_v[span, :])
            up_act += dot(piece, wup_v[span, :])
        if i < 1:
            acc_v[0] = gate_act
            acc_v[1] = up_act
            gate_act, up_act = acc_v[0], acc_v[1]
    inv_ffn = lax.rsqrt(square / model_width + epsilon)
    gate_act = gate_act * inv_ffn
    up_act = up_act * inv_ffn
    hidden = (gate_act / (1.0 + jnp.exp(-gate_act)) * up_act).astype(bf16)
    loaded(wdown_v, 9)
    def deliver(pair, results):
        for r, result in zip(pair, results):
            down_src[r] = result.astype(bf16)
        for r in pair:
            remote(down_src.at[r], down_rx.at[slot(r)], 6, last, r)

    order = near[::-1]
    pending = None
    for first in range(0, count - 1, 2):
        pair = order[first : first + 2]
        results = [dot(hidden, wdown_v[place(r)]) for r in pair]
        if pending:
            deliver(*pending)
        pending = (pair, results)
    total = dot(hidden, wdown_v[me])
    deliver(*pending)
    residual = resid_rx[block, :, pl.ds(pl.multiple_of(tp * out_block, out_block), out_block)]
    total += residual.astype(f32)

    def first_sent():
        sent(small_rx.at[pl.ds(1, blocks - 1)], 0)
        sent(q_rx.at[pl.ds(1, blocks - 1)], 0)
        sent(kv_rx.at[pl.ds(1, blocks - 1)], 0)

    @pl.when(jnp.logical_and(early, follows))
    def _():
        sent(small_src, 0)
        sent(q_src, 0)
        sent(kv_src, 0)

    pl.when(jnp.logical_and(early, leads))(first_sent)
    pl.when(jnp.logical_or(kv != 0, leads))(first_sent)

    @pl.when(leads)
    def _():
        for _ in range(count_tp):
            sent(resid_rx.at[pl.ds(0, blocks - 1)], 5)
        sent(resid_rx.at[pl.ds(0, count_tp - 1)], 5)

    arrived(down_rx.at[pl.ds(1, count - 1)], last)
    for r in near:
        total += down_rx[r].astype(f32)
    out_ref[...] = total.astype(bf16)
    sent(down_rx.at[pl.ds(1, count - 1)], 6)


def fused(
    tokens, lengths, cache_keys, cache_values, cache_igate, cache_fcum, gain_mix,
    w_query, w_key, w_value, w_gates, w_out, gain_ffn, w_gate, w_up, w_down,
):
    sizes = tuple(lax.axis_size(name) for name in ("dp", "kv", "tp"))
    count = sizes[0] * sizes[1] * sizes[2]
    blocks = sizes[0] * sizes[1]
    f32, bf16 = jnp.float32, jnp.bfloat16
    rows, feat = tokens.shape
    seqs, block_len, heads, key_size = cache_keys.shape
    value_size = cache_values.shape[3]
    out_block = w_out.shape[1]
    half_kv = heads * (key_size + value_size) // 2
    width_v = heads * value_size
    hbm = pl.BlockSpec(memory_space=pl.ANY)
    vmem = pl.BlockSpec(memory_space=pltpu.VMEM)
    dma = pltpu.SemaphoreType.DMA
    scratch = [
        pltpu.SMEM((seqs,), jnp.int32),
        pltpu.VMEM(tokens.shape, bf16),
        pltpu.VMEM((heads, seqs, block_len), f32),
        pltpu.VMEM((heads, seqs, block_len), f32),
        pltpu.VMEM((2, blocks * feat // 128, 128), bf16),
        pltpu.VMEM(w_query.shape, bf16),
        pltpu.VMEM(w_key.shape, bf16),
        pltpu.VMEM(w_value.shape, bf16),
        pltpu.VMEM((w_gates.shape[1], feat), bf16),
        pltpu.VMEM((sizes[2],) + w_out.shape, bf16),
        pltpu.VMEM(w_gate.shape, bf16),
        pltpu.VMEM(w_up.shape, bf16),
        pltpu.VMEM((count, w_down.shape[0], out_block), bf16),
        pltpu.VMEM((heads, seqs * block_len, key_size), bf16),
        pltpu.VMEM((heads, seqs * block_len, value_size), bf16),
        pltpu.VMEM((heads, key_size, seqs * block_len), bf16),
        pltpu.VMEM((sizes[0], seqs, heads * key_size), bf16),
        pltpu.VMEM((rows, 2, half_kv), bf16),
        pltpu.VMEM((sizes[0], 1, 128), f32),
        pltpu.VMEM((blocks, seqs, heads * key_size), bf16),
        pltpu.VMEM((blocks, 2, half_kv), bf16),
        pltpu.VMEM((blocks, 1, 128), f32),
        pltpu.VMEM((sizes[0], seqs, heads * key_size), bf16),
        pltpu.VMEM((rows, 2, half_kv), bf16),
        pltpu.VMEM((sizes[0], 1, 128), f32),
        pltpu.VMEM((2, rows, w_gate.shape[1]), f32),
        pltpu.VMEM((seqs, width_v + 128), f32),
        pltpu.VMEM((seqs, width_v + 128), bf16),
        pltpu.VMEM((sizes[2] * sizes[1], seqs, width_v + 128), bf16),
        pltpu.VMEM((sizes[0], seqs, sizes[2] * width_v), bf16),
        pltpu.VMEM((blocks, rows, feat), bf16),
        pltpu.VMEM((count, rows, out_block), bf16),
        pltpu.VMEM((count, rows, out_block), bf16),
        pltpu.VMEM((2, blocks * feat // 128, 128), f32),
        dma((10,)),
        dma((1,)),
        dma((5 + sizes[0] + sizes[1] - 1 + 5,)),
    ]
    operands = (
        lengths, tokens, cache_igate.swapaxes(0, 1), cache_fcum.swapaxes(0, 1),
        gain_mix.reshape(-1, 128), gain_ffn.reshape(-1, 128),
        cache_keys.swapaxes(1, 2), cache_values.swapaxes(1, 2),
        w_query, w_key, w_value, w_gates.T, w_out, w_gate, w_up, w_down,
    )
    return pl.pallas_call(
        functools.partial(fused_kernel, sizes),
        out_shape=pltpu.VMEM((rows, out_block), bf16),
        in_specs=[hbm] * len(operands),
        out_specs=vmem,
        scratch_shapes=scratch,
        compiler_params=pltpu.CompilerParams(
            collective_id=0, has_side_effects=True, vmem_limit_bytes=40 * 1024 * 1024
        ),
    )(*[pltpu.with_memory_space_constraint(x, pltpu.HBM) for x in operands])


def fits_kernel(tokens, cache_keys, w_out, w_gate):
    return (
        cache_keys.shape[0] == lax.axis_size("kv")
        and all(n in (2, 4) for n in map(lax.axis_size, ("dp", "kv")))
        and lax.axis_size("tp") == 2
        and cache_keys.shape[2] <= 3
        and tokens.shape[1] % 128 == 0
        and w_out.shape[1] % 128 == 0
        and w_gate.shape[1] % 128 == 0
    )


def layer(*args):
    if fits_kernel(args[0], args[2], args[11], args[13]):
        return fused(*args)
    return per_device(*args)


def solution(mesh):
    in_specs = (
        P("grp", ("dp", "kv")),
        P(("grp", "dp")),
        P(("grp", "dp"), "kv", "tp", None),
        P(("grp", "dp"), "kv", "tp", None),
        P(("grp", "dp"), "tp", "kv"),
        P(("grp", "dp"), "tp", "kv"),
        P(),
        P(("dp", "kv"), "tp"),
        P(("dp", "kv"), "tp"),
        P(("dp", "kv"), "tp"),
        P(),
        P(None, ("dp", "kv", "tp")),
        P(),
        P(None, ("dp", "kv", "tp")),
        P(None, ("dp", "kv", "tp")),
        P(("dp", "kv", "tp"), None),
    )
    out_specs = P("grp", ("dp", "kv", "tp"))
    return jax.shard_map(
        layer, mesh=mesh, in_specs=in_specs, out_specs=out_specs, check_vma=False
    )
```
